32 devices in a mesh: grp: 2 (over y), sp: 4 (over z), fs: 2 (over x), tp: 2 (over core).
Axes of the slice: x: 2, y: 2, z: 4, core: 2. Of those that a mesh axis runs over, the one named last changes fastest.
Arguments:
- tokens: bfloat16 [4, 512, 2048], P(('grp', 'fs'), 'sp', 'tp'), parts along dimension 0, may hold values from -120 to 120
- mix_gain: float32 [2048], replicated, may hold values from 0.1 to 1.9
- attn_query: bfloat16 [2048, 1024], P('fs', 'tp'), may hold values from -0.375 to 0.375
- attn_key: bfloat16 [2048, 1024], P('fs', 'tp'), may hold values from -0.125 to 0.125
- attn_value: bfloat16 [2048, 1024], P('fs', 'tp'), may hold values from -0.125 to 0.125
- rec_query: bfloat16 [2048, 1024], P('fs', 'tp'), may hold values from -0.125 to 0.125
- rec_forget: bfloat16 [2048, 1024], P('fs', 'tp'), may hold values from -0.125 to 0.125
- rec_input: bfloat16 [2048, 1024], P('fs', 'tp'), may hold values from -0.125 to 0.125
- break_offset: float32 [8], P('tp'), may hold values from -13.5 to -7
- forget_room: float32 [8, 128], P('tp'), may hold values from 0.0009765625 to 0.05
- out_gain: float32 [128], replicated, may hold values from 0.1 to 1.9
- out_attn: bfloat16 [1024, 2048], P('tp', 'fs'), may hold values from -0.125 to 0.125
- out_rec: bfloat16 [1024, 2048], P('tp', 'fs'), may hold values from -0.125 to 0.125
Outputs:
- mixed: bfloat16 [4, 512, 2048], P(('grp', 'fs'), ('sp', 'tp')), parts along dimension 0
The draws below stay inside these ranges and needn't reach their ends.
There are 2 independent parts, one for each index of `grp`. The reference program is written for one: setup_inputs(seed, part) draws one part's arguments, and reference() takes and returns one part's arrays. A program takes and returns all parts, laid end to end along the dimension named above; an argument that names none is the same for every part. Nothing has to cross between parts.
All inputs are finite; a program needn't handle non-finite values.
Results may differ from the reference program's by a relative error of at most 0.019.
Values may be sent and summed in bfloat16 or wider, within the bound.
A program may use at most 64 MiB of HBM per device.

```python
import math
import jax
import jax.numpy as jnp
from jax import lax

D = 2048
SB_HEADS = 8
HEAD = 128
REC_HEADS = 8
DK = 128
DV = 128
REC_BLOCK = 64
TOK_DEV = 128
SEQS = 2
LENGTH = 512
N_TP = 2


def draw_tokens(key, part):
    full_shape = (SEQS, LENGTH, D)
    subkeys = jax.random.split(key, 4)
    row_scale = jnp.exp(jax.random.uniform(subkeys[0], (SEQS, LENGTH, 1), jnp.float32, 0.0, math.log(10.0)))
    col_scale = jnp.exp(jax.random.uniform(subkeys[1], (1, 1, D), jnp.float32, 0.0, math.log(10.0)))
    regions = jax.random.normal(subkeys[2], (SEQS, LENGTH // TOK_DEV, 1, D), jnp.float32)
    regions = jnp.broadcast_to(regions, (SEQS, LENGTH // TOK_DEV, TOK_DEV, D)).reshape(full_shape)
    rough_part = jax.random.normal(subkeys[3], full_shape, jnp.float32)
    regions = 0.5 * regions
    drawn = (rough_part * col_scale / 3.0 + regions) * row_scale
    return jnp.clip(drawn, -120.0, 120.0).astype(jnp.bfloat16)


def block_scale(key, extent, shards, smallest, high):
    level, own = 1.0, jax.random.fold_in(key, 6)
    for position, blocks in shards:
        heights = jnp.exp(jax.random.uniform(jax.random.fold_in(own, position), (blocks,), jnp.float32, smallest / len(shards), high / len(shards)))
        level = level * jnp.repeat(heights, extent[position] // blocks).reshape([-1 if axis == position else 1 for axis in range(len(extent))])
    return level


def normal_values(stream_key, shape, width, bound, cuts=(), kind=jnp.bfloat16):
    entries = jax.random.normal(stream_key, shape, jnp.float32) * width
    if len(cuts) > 0:
        entries = block_scale(stream_key, shape, cuts, -0.22, 0.18) * entries
    return jnp.clip(entries, min=-bound, max=bound).astype(kind)


def setup_inputs(seed: int = 0, part: int = 0) -> dict:
    arg_keys = jax.random.split(jax.random.key(seed), 14)
    part_keys = jax.random.split(jax.random.fold_in(arg_keys[13], part), 14)
    tokens = draw_tokens(jax.random.fold_in(jax.random.fold_in(arg_keys[13], part), 71), part)
    mix_gain = jnp.clip(1.0 + 0.18 * jax.random.normal(arg_keys[1], (D,), jnp.float32), 0.1, 1.9)
    attn_query = normal_values(arg_keys[2], (D, SB_HEADS * HEAD), (D // 9) ** -0.5, 0.375, ((0, 2), (1, 2)))
    attn_key = normal_values(arg_keys[3], (D, SB_HEADS * HEAD), D ** -0.5, 0.125, ((0, 2), (1, 2)))
    attn_value = normal_values(arg_keys[4], (D, SB_HEADS * HEAD), D ** -0.5, 0.125, ((0, 2), (1, 2)))
    rec_query = normal_values(arg_keys[5], (D, REC_HEADS * DK), D ** -0.5, 0.125, ((0, 2), (1, 2)))
    rec_forget = normal_values(arg_keys[6], (D, REC_HEADS * DK), D ** -0.5, 0.125, ((0, 2), (1, 2)))
    rec_input = normal_values(arg_keys[7], (D, REC_HEADS * DV), D ** -0.5, 0.125, ((0, 2), (1, 2)))
    break_offset = jnp.clip(-13.5 + 6.5 * jax.random.uniform(arg_keys[8], (SB_HEADS,), jnp.float32) ** block_scale(arg_keys[8], (SB_HEADS,), ((0, 2),), -0.2, 0.2), -13.5, -7.0)
    forget_room = jnp.clip(jnp.exp(math.log(0.05) - 3.9357395 * jax.random.uniform(arg_keys[9], (REC_HEADS, DK), jnp.float32) ** block_scale(arg_keys[9], (REC_HEADS, DK), ((0, 2),), -0.2, 0.2)), 0.0009765625, 0.05)
    out_gain = jnp.clip(1.0 + 0.18 * jax.random.normal(arg_keys[10], (DV,), jnp.float32), 0.1, 1.9)
    out_attn = normal_values(arg_keys[11], (SB_HEADS * HEAD, D), (SB_HEADS * HEAD + REC_HEADS * DV) ** -0.5, 0.125, ((0, 2), (1, 2)))
    out_rec = normal_values(arg_keys[12], (REC_HEADS * DV, D), (SB_HEADS * HEAD + REC_HEADS * DV) ** -0.5, 0.125, ((0, 2), (1, 2)))
    return {"tokens": tokens, "mix_gain": mix_gain, "attn_query": attn_query, "attn_key": attn_key, "attn_value": attn_value, "rec_query": rec_query, "rec_forget": rec_forget, "rec_input": rec_input, "break_offset": break_offset, "forget_room": forget_room, "out_gain": out_gain, "out_attn": out_attn, "out_rec": out_rec}


norm_eps = 1e-06
highest = lax.Precision.HIGHEST

def block_step(states, inputs):
    queries, key_in, value_rows, log_forget = inputs
    block_len = queries.shape[-2]
    cum_log = jnp.cumsum(log_forget, axis=-2)
    last_log = cum_log[..., -1:, :]
    q_dec = queries * jnp.exp(cum_log)
    k_inv = key_in * jnp.exp(-cum_log)
    causal = lax.iota(jnp.int32, block_len)[:, None] >= lax.iota(jnp.int32, block_len)[None, :]
    carried_part = jnp.einsum('...tk,...kv->...tv', q_dec, states, precision=highest)
    scores = jnp.where(causal, jnp.einsum('...tk,...sk->...ts', q_dec, k_inv, precision=highest), 0.0)
    inner_part = jnp.einsum('...ts,...sv->...tv', scores, value_rows, precision=highest)
    fresh_state = jnp.einsum('...sk,...sv->...kv', key_in * jnp.exp(last_log - cum_log), value_rows, precision=highest)
    return (jnp.exp(jnp.swapaxes(last_log, -1, -2)) * states + fresh_state, carried_part + inner_part)

def stick_sequence(queries, key_rows, value_rows, offsets):
    head_count = queries.shape[1]
    head_width = queries.shape[2]
    factor = 1.0 / math.sqrt(head_width)
    blocks = LENGTH // TOK_DEV

    def per_block(block_idx):
        q_blk = lax.dynamic_slice_in_dim(queries, block_idx * TOK_DEV, TOK_DEV, 0).astype(jnp.float32)
        q_pos = block_idx * TOK_DEV + lax.iota(jnp.int32, TOK_DEV)

        def turn(step_idx, carried):
            sums_acc, running = carried
            source = block_idx - step_idx
            k_blk = lax.dynamic_slice_in_dim(key_rows, source * TOK_DEV, TOK_DEV, 0).astype(jnp.float32)
            v_blk = lax.dynamic_slice_in_dim(value_rows, source * TOK_DEV, TOK_DEV, 0).astype(jnp.float32)
            scores = jnp.einsum('qhe,khe->hqk', q_blk, k_blk) * factor + offsets[:, None, None]
            k_pos = source * TOK_DEV + lax.iota(jnp.int32, TOK_DEV)
            strict = k_pos[None, :] < q_pos[:, None]
            log_keep = jnp.where(strict, jax.nn.log_sigmoid(-scores), 0.0)
            inner_sum = lax.cumsum(log_keep, axis=2, reverse=True) - log_keep
            sticks = jnp.where(strict, jnp.exp(jax.nn.log_sigmoid(scores) + inner_sum), 0.0)
            sticks = lax.optimization_barrier(sticks.astype(jnp.bfloat16)).astype(jnp.float32)
            partial_value = jnp.einsum('hqk,khe->qhe', sticks, v_blk)
            sums_acc = sums_acc + partial_value * jnp.transpose(jnp.exp(running))[:, :, None]
            return (sums_acc, running + lax.optimization_barrier(jnp.sum(log_keep, axis=2)))
        start_state = (jnp.zeros((TOK_DEV, head_count, head_width), jnp.float32), jnp.zeros((head_count, TOK_DEV), jnp.float32))
        sums_acc, unused_run = lax.fori_loop(0, block_idx + 1, turn, start_state)
        return sums_acc.astype(jnp.bfloat16)
    result = lax.map(per_block, jnp.arange(blocks, dtype=jnp.int32))
    return result.reshape(LENGTH, head_count, head_width)

def recur_sequence(queries, gate_pre, inputs, rooms, gain):
    key_in = rooms * jax.nn.sigmoid(-gate_pre.astype(jnp.float32))
    log_forget = jnp.log1p(-key_in)
    head_count = queries.shape[1]
    blocks = LENGTH // REC_BLOCK

    def split_blocks(tensor):
        return jnp.transpose(tensor.reshape(blocks, REC_BLOCK, head_count, tensor.shape[2]), (0, 2, 1, 3))
    empty_state = jnp.zeros((head_count, DK, DV), jnp.float32)
    final_state, pieces = lax.scan(block_step, empty_state, (split_blocks(queries.astype(jnp.float32)), split_blocks(key_in), split_blocks(inputs.astype(jnp.float32)), split_blocks(log_forget)))
    raw_out = jnp.transpose(pieces, (0, 2, 1, 3)).reshape(LENGTH, head_count, DV)
    factor = lax.rsqrt(lax.optimization_barrier(jnp.mean(raw_out * raw_out, axis=2, keepdims=True)) + norm_eps)
    return (raw_out * factor * gain).astype(jnp.bfloat16)

def reference(tokens, mix_gain, attn_query, attn_key, attn_value, rec_query, rec_forget, rec_input, break_offset, forget_room, out_gain, out_attn, out_rec):
    rows32 = tokens.astype(jnp.float32)
    factor = lax.rsqrt(lax.optimization_barrier(jnp.mean(rows32 * rows32, axis=2, keepdims=True)) + norm_eps)
    normed = (rows32 * factor * mix_gain).astype(jnp.bfloat16).reshape(SEQS * LENGTH, D)

    def project(matrix, head_width):
        product = jnp.dot(normed, matrix, preferred_element_type=jnp.float32).astype(jnp.bfloat16)
        return product.reshape(SEQS, LENGTH, matrix.shape[1] // head_width, head_width)
    attn_q = project(attn_query, HEAD)
    attn_k = project(attn_key, HEAD)
    attn_v = project(attn_value, HEAD)
    rec_q = project(rec_query, DK)
    rec_f = project(rec_forget, DK)
    rec_i = project(rec_input, DV)
    attn_out = lax.map(lambda triple: stick_sequence(triple[0], triple[1], triple[2], break_offset), (attn_q, attn_k, attn_v))
    rec_out = lax.map(lambda triple: recur_sequence(triple[0], triple[1], triple[2], forget_room, out_gain), (rec_q, rec_f, rec_i))
    attn_flat = attn_out.reshape(SEQS * LENGTH, SB_HEADS * HEAD)
    rec_flat = rec_out.reshape(SEQS * LENGTH, REC_HEADS * DV)
    attn_part = SB_HEADS * HEAD // N_TP
    rec_part = REC_HEADS * DV // N_TP
    mixed = jnp.zeros((SEQS * LENGTH, D), jnp.float32)
    for group in range(N_TP):
        attn_slice = attn_flat[:, group * attn_part:(group + 1) * attn_part]
        rec_slice = rec_flat[:, group * rec_part:(group + 1) * rec_part]
        partial_value = jnp.dot(attn_slice, out_attn[group * attn_part:(group + 1) * attn_part], preferred_element_type=jnp.float32) + jnp.dot(rec_slice, out_rec[group * rec_part:(group + 1) * rec_part], preferred_element_type=jnp.float32)
        mixed = mixed + lax.optimization_barrier(partial_value.astype(jnp.bfloat16)).astype(jnp.float32)
    return mixed.astype(jnp.bfloat16).reshape(SEQS, LENGTH, D)
```

```python
import functools
import math

import jax
import jax.numpy as jnp
from jax import lax
from jax.experimental import pallas as pl
from jax.experimental.pallas import tpu as pltpu
from jax.sharding import PartitionSpec as P

LANES = 128
norm_eps = 1e-06
MESH = pl.DeviceIdType.MESH
F32 = jnp.float32
BF16 = jnp.bfloat16
N_PROJ = 6


def dot_nn(a, b):
    return lax.dot_general(a, b, (((1,), (0,)), ((), ())), preferred_element_type=F32)


def dot_nt(a, b):
    return lax.dot_general(a, b, (((1,), (1,)), ((), ())), preferred_element_type=F32)


def dot_tn(a, b):
    return lax.dot_general(a, b, (((0,), (0,)), ((), ())), preferred_element_type=F32)


def halves(x):
    high = x.astype(BF16)
    return high, (x - high.astype(F32)).astype(BF16)


def kernel(
    n_sp, n_fs, n_tp,
    tok, gain, w_k, w_v, w_f, w_i, w_q, w_r, offs, room, out_gain, o_attn, o_rec,
    out,
    wbuf, obuf, xt, xg, ss, acc, psend, precv, kv, qbuf, qdec, ecum, kinv,
    att, run, loc, st_loc, dec, st_in, st_out, heads, hrecv, part, precv2, mix, mrecv,
    w_sem, x_send, x_recv, ss_send, ss_recv, p_send, p_recv, kv_send, kv_recv,
    st_sem, h_send, h_recv, pp_send, pp_recv, m_send, m_recv,
):
    sp, fs, tp = lax.axis_index("sp"), lax.axis_index("fs"), lax.axis_index("tp")
    rows, feat_t = tok.shape
    feat_f = xt.shape[2]
    width = feat_t * n_tp
    cols = wbuf.shape[2]
    n_heads = cols // LANES
    share = rows // n_tp
    out_cols = obuf.shape[2]
    has_next = sp < n_sp - 1
    has_prev = sp > 0

    def fs_at(step):
        return lax.rem(fs + step, n_fs)

    def tp_at(step):
        return lax.rem(tp + step, n_tp)

    w_copies = [
        pltpu.make_async_copy(w, wbuf.at[i], w_sem.at[i])
        for i, w in enumerate((w_k, w_v, w_f, w_i, w_q, w_r))
    ]
    w_copies += [
        pltpu.make_async_copy(w, obuf.at[i], w_sem.at[N_PROJ + i])
        for i, w in enumerate((o_attn, o_rec))
    ]
    for copy in w_copies:
        copy.start()

    barrier = pltpu.get_barrier_semaphore()
    for df in range(n_fs):
        for dt in range(n_tp):
            if df or dt:
                pl.semaphore_signal(
                    barrier, inc=1, device_id={"fs": fs_at(df), "tp": tp_at(dt)}, device_id_type=MESH
                )

    @pl.when(has_next)
    def _():
        pl.semaphore_signal(barrier, inc=1, device_id={"sp": sp + 1}, device_id_type=MESH)

    @pl.when(has_prev)
    def _():
        pl.semaphore_signal(barrier, inc=1, device_id={"sp": sp - 1}, device_id_type=MESH)

    squares = jnp.zeros((rows, LANES), F32)
    for c in range(feat_t // LANES):
        piece = tok[:, c * LANES:(c + 1) * LANES].astype(F32)
        squares = squares + piece * piece
    ss[tp] = squares

    next_count = jnp.where(has_next, 1, 0)
    prev_count = jnp.where(has_prev, 1, 0)
    pl.semaphore_wait(barrier, n_fs * n_tp - 1 + next_count + prev_count)

    def holder(f_index):
        return (f_index * feat_f) // feat_t

    def x_copy(df, dt):
        dest = fs_at(df)
        start = pl.multiple_of(lax.rem(dest * feat_f, feat_t), LANES)
        return pltpu.make_async_remote_copy(
            src_ref=tok.at[:, pl.ds(start, feat_f)],
            dst_ref=xt.at[fs],
            send_sem=x_send.at[df * n_tp + dt],
            recv_sem=x_recv.at[fs],
            device_id={"fs": dest, "tp": tp_at(dt)},
            device_id_type=MESH,
        )

    x_order = [(df, dt) for df in list(range(1, n_fs)) + [0] for dt in range(n_tp) if df or dt]
    for df, dt in x_order:
        @pl.when(holder(fs_at(df)) == tp)
        def _(df=df, dt=dt):
            x_copy(df, dt).start()

    def ss_copy(dt):
        return pltpu.make_async_remote_copy(
            src_ref=ss.at[tp], dst_ref=ss.at[tp],
            send_sem=ss_send.at[dt - 1], recv_sem=ss_recv.at[tp],
            device_id={"tp": tp_at(dt)}, device_id_type=MESH,
        )

    for dt in range(1, n_tp):
        ss_copy(dt).start()

    own_holder = holder(fs) == tp
    gain_f = gain[:, pl.ds(pl.multiple_of(fs * feat_f, LANES), feat_f)]

    @pl.when(own_holder)
    def _():
        start = pl.multiple_of(lax.rem(fs * feat_f, feat_t), LANES)
        xg[0] = (tok[:, pl.ds(start, feat_f)].astype(F32) * gain_f).astype(BF16)

    def x_wait(slot):
        pltpu.make_async_remote_copy(
            src_ref=xt.at[slot], dst_ref=xt.at[slot],
            send_sem=x_send.at[0], recv_sem=x_recv.at[slot],
            device_id={"tp": tp_at(1)}, device_id_type=MESH,
        ).wait_recv()

    def p_copy(df, w):
        return pltpu.make_async_remote_copy(
            src_ref=psend.at[df - 1, w], dst_ref=precv.at[df - 1, w],
            send_sem=p_send.at[(df - 1) * N_PROJ + w], recv_sem=p_recv.at[(df - 1) * N_PROJ + w],
            device_id={"fs": fs_at(df)}, device_id_type=MESH,
        )

    for df in range(1, n_fs):
        slot = fs_at(df)
        x_wait(slot)
        xg[df] = (xt[slot].astype(F32) * gain_f).astype(BF16)
    for w in range(N_PROJ):
        w_copies[w].wait()
        for df in range(1, n_fs):
            psend[df - 1, w] = dot_nn(xg[df], wbuf[w]).astype(BF16)
            p_copy(df, w).start()

    @pl.when(jnp.logical_not(own_holder))
    def _():
        x_wait(fs)
        xg[0] = (xt[fs].astype(F32) * gain_f).astype(BF16)

    for w in range(N_PROJ):
        acc[w] = dot_nn(xg[0], wbuf[w])

    total = ss[tp]
    for dt in range(1, n_tp):
        other = tp_at(dt)
        pltpu.make_async_remote_copy(
            src_ref=ss.at[other], dst_ref=ss.at[other],
            send_sem=ss_send.at[dt - 1], recv_sem=ss_recv.at[other],
            device_id={"tp": other}, device_id_type=MESH,
        ).wait_recv()
        total = total + ss[other]
    factor = lax.rsqrt(jnp.sum(total, axis=1, keepdims=True) / width + norm_eps)

    def finish(w):
        value = acc[w]
        for df in range(1, n_fs):
            p_copy(df, w).wait_recv()
            value = value + precv[df - 1, w].astype(F32)
        return (value * factor).astype(BF16)

    def kv_copy(slot, c):
        return pltpu.make_async_remote_copy(
            src_ref=kv.at[slot, c], dst_ref=kv.at[slot, c],
            send_sem=kv_send.at[slot * 2 + c], recv_sem=kv_recv.at[slot * 2 + c],
            device_id={"sp": lax.rem(sp + 1, n_sp)}, device_id_type=MESH,
        )

    for c in range(2):
        kv[sp, c] = finish(c)

        @pl.when(has_next)
        def _(c=c):
            kv_copy(sp, c).start()

    iota_r = lax.broadcasted_iota(jnp.int32, (rows, rows), 0)
    iota_c = lax.broadcasted_iota(jnp.int32, (rows, rows), 1)
    causal = iota_r >= iota_c
    strict = iota_c < iota_r

    def st_copy():
        return pltpu.make_async_remote_copy(
            src_ref=st_out, dst_ref=st_in, send_sem=st_sem.at[0], recv_sem=st_sem.at[1],
            device_id={"sp": lax.rem(sp + 1, n_sp)}, device_id_type=MESH,
        )

    lower = jnp.where(causal, 1.0, 0.0).astype(BF16)
    forget_pre = finish(2)
    rec_i = finish(3)
    for h in range(n_heads):
        lanes = slice(h * LANES, (h + 1) * LANES)
        key_in = room[h:h + 1, :] * jax.nn.sigmoid(-forget_pre[:, lanes].astype(F32))
        high, low = halves(jnp.log1p(-key_in))
        cum = dot_nn(lower, high) + dot_nn(lower, low)
        last = cum[rows - 1:rows, :]
        ecum[:, lanes] = jnp.exp(cum)
        kinv[:, lanes] = (key_in * jnp.exp(-cum)).astype(BF16)
        fresh = (key_in * jnp.exp(last - cum)).astype(BF16)
        st_loc[h] = dot_tn(rec_i[:, lanes], fresh)
        dec[h] = jnp.broadcast_to(jnp.exp(last), dec.shape[1:])

    @pl.when(jnp.logical_and(sp == 0, has_next))
    def _():
        st_out[...] = st_loc[...].astype(BF16)
        st_copy().start()

    qbuf[...] = finish(4)
    later = jnp.where(iota_r > iota_c, 1.0, 0.0).astype(BF16)
    sums = jnp.concatenate([later, jnp.ones((rows, LANES), BF16)], axis=1)
    scale = 1.0 / math.sqrt(LANES)

    def attend(slot, diagonal):
        for h in range(n_heads):
            lanes = slice(h * LANES, (h + 1) * LANES)
            z = dot_nt(qbuf[:, lanes], kv[slot, 0, :, lanes]) * scale + offs[h]
            keep = -(jnp.maximum(z, 0.0) + jnp.log1p(jnp.exp(-jnp.abs(z))))
            log_stick = z + keep
            if diagonal:
                keep = jnp.where(strict, keep, 0.0)
            high, low = halves(keep)
            both = dot_nn(high, sums) + dot_nn(low, sums)
            stick = jnp.exp(log_stick + both[:, :rows])
            if diagonal:
                stick = jnp.where(strict, stick, 0.0)
            value = dot_nn(stick.astype(BF16), kv[slot, 1, :, lanes])
            if diagonal:
                att[:, lanes] = value
                run[h] = both[:, rows:]
            else:
                past = run[h]
                att[:, lanes] += value * jnp.exp(past)
                run[h] = past + both[:, rows:]

    attend(sp, True)

    rec_q = finish(5)
    for h in range(n_heads):
        lanes = slice(h * LANES, (h + 1) * LANES)
        decayed = (rec_q[:, lanes].astype(F32) * ecum[:, lanes]).astype(BF16)
        qdec[:, lanes] = decayed
        scores = jnp.where(causal, dot_nt(decayed, kinv[:, lanes]), 0.0)
        loc[:, lanes] = dot_nn(scores.astype(BF16), rec_i[:, lanes])

    def block(step, carry):
        slot = sp - step
        for c in range(2):
            kv_copy(slot, c).wait_recv()

            @pl.when(has_next)
            def _(c=c):
                kv_copy(slot, c).start()
        attend(slot, False)
        return carry

    lax.fori_loop(1, sp + 1, block, 0)

    def h_copy(df, c):
        return pltpu.make_async_remote_copy(
            src_ref=heads.at[c], dst_ref=hrecv.at[df - 1, c],
            send_sem=h_send.at[(df - 1) * 2 + c], recv_sem=h_recv.at[(df - 1) * 2 + c],
            device_id={"fs": fs_at(df)}, device_id_type=MESH,
        )

    heads[0] = att[...].astype(BF16)
    for df in range(1, n_fs):
        h_copy(df, 0).start()

    @pl.when(has_prev)
    def _():
        st_copy().wait_recv()

        @pl.when(has_next)
        def _():
            for h in range(n_heads):
                st_out[h] = (st_in[h].astype(F32) * dec[h, 0:1, :] + st_loc[h]).astype(BF16)
            st_copy().start()

        for h in range(n_heads):
            lanes = slice(h * LANES, (h + 1) * LANES)
            loc[:, lanes] += dot_nt(qdec[:, lanes], st_in[h])

    for h in range(n_heads):
        lanes = slice(h * LANES, (h + 1) * LANES)
        raw = loc[:, lanes]
        norm = lax.rsqrt(jnp.mean(raw * raw, axis=1, keepdims=True) + norm_eps)
        heads[1, :, lanes] = (raw * norm * out_gain[...]).astype(BF16)
    for df in range(1, n_fs):
        h_copy(df, 1).start()

    w_copies[N_PROJ].wait()
    w_copies[N_PROJ + 1].wait()

    def pp_copy(df, dt):
        index = df * (n_tp - 1) + dt - 1
        start = pl.multiple_of(tp_at(dt) * share, share)
        return pltpu.make_async_remote_copy(
            src_ref=part.at[df, pl.ds(start, share)], dst_ref=precv2.at[dt - 1, df],
            send_sem=pp_send.at[index], recv_sem=pp_recv.at[index],
            device_id={"tp": tp_at(dt)}, device_id_type=MESH,
        )

    def m_copy(df):
        return pltpu.make_async_remote_copy(
            src_ref=mix.at[df - 1], dst_ref=mrecv.at[df - 1],
            send_sem=m_send.at[df - 1], recv_sem=m_recv.at[df - 1],
            device_id={"fs": fs_at(df)}, device_id_type=MESH,
        )

    def project(df, first, second):
        part[df] = (dot_nn(first, obuf[0]) + dot_nn(second, obuf[1])).astype(BF16)
        for dt in range(1, n_tp):
            pp_copy(df, dt).start()

    def reduced(df):
        value = part[df, pl.ds(pl.multiple_of(tp * share, share), share)].astype(F32)
        for dt in range(1, n_tp):
            pp_copy(df, dt).wait_recv()
            value = value + precv2[dt - 1, df].astype(F32)
        return value.astype(BF16)

    project(0, heads[0], heads[1])
    for df in range(1, n_fs):
        h_copy(df, 0).wait_recv()
        h_copy(df, 1).wait_recv()
        project(df, hrecv[df - 1, 0], hrecv[df - 1, 1])
    for df in range(1, n_fs):
        mix[df - 1] = reduced(df)
        m_copy(df).start()
    out[:, pl.ds(pl.multiple_of(fs * out_cols, LANES), out_cols)] = reduced(0)
    for df in range(1, n_fs):
        m_copy(df).wait_recv()
        source = lax.rem(fs + n_fs - df, n_fs)
        out[:, pl.ds(pl.multiple_of(source * out_cols, LANES), out_cols)] = mrecv[df - 1]

    for df, dt in x_order:
        @pl.when(holder(fs_at(df)) == tp)
        def _(df=df, dt=dt):
            x_copy(df, dt).wait_send()
    for dt in range(1, n_tp):
        ss_copy(dt).wait_send()
    for df in range(1, n_fs):
        for w in range(N_PROJ):
            p_copy(df, w).wait_send()
        for c in range(2):
            h_copy(df, c).wait_send()
        m_copy(df).wait_send()
    for df in range(n_fs):
        for dt in range(1, n_tp):
            pp_copy(df, dt).wait_send()

    @pl.when(has_next)
    def _():
        st_copy().wait_send()

        def drain(slot, carry):
            for c in range(2):
                kv_copy(slot, c).wait_send()
            return carry

        lax.fori_loop(0, sp + 1, drain, 0)


def body(
    tokens, mix_gain, attn_query, attn_key, attn_value, rec_query, rec_forget, rec_input,
    break_offset, forget_room, out_gain, out_attn, out_rec,
):
    n_sp, n_fs, n_tp = lax.axis_size("sp"), lax.axis_size("fs"), lax.axis_size("tp")
    rows, feat_t = tokens.shape[1], tokens.shape[2]
    feat_f, cols = attn_query.shape
    width = feat_t * n_tp
    n_heads = cols // LANES
    out_rows, out_cols = out_attn.shape
    share = rows // n_tp
    vmem = pl.BlockSpec(memory_space=pltpu.VMEM)
    smem = pl.BlockSpec(memory_space=pltpu.SMEM)
    hbm = pl.BlockSpec(memory_space=pl.ANY)
    dma = pltpu.SemaphoreType.DMA
    square = (n_heads, LANES, LANES)
    result = pl.pallas_call(
        functools.partial(kernel, n_sp, n_fs, n_tp),
        out_shape=jax.ShapeDtypeStruct((share, width), BF16),
        in_specs=[vmem, vmem] + [hbm] * 6 + [smem, vmem, vmem, hbm, hbm],
        out_specs=vmem,
        scratch_shapes=[
            pltpu.VMEM((N_PROJ, feat_f, cols), BF16),
            pltpu.VMEM((2, out_rows, out_cols), BF16),
            pltpu.VMEM((n_fs, rows, feat_f), BF16),
            pltpu.VMEM((n_fs, rows, feat_f), BF16),
            pltpu.VMEM((n_tp, rows, LANES), F32),
            pltpu.VMEM((N_PROJ, rows, cols), F32),
            pltpu.VMEM((n_fs - 1, N_PROJ, rows, cols), BF16),
            pltpu.VMEM((n_fs - 1, N_PROJ, rows, cols), BF16),
            pltpu.VMEM((n_sp, 2, rows, cols), BF16),
            pltpu.VMEM((rows, cols), BF16),
            pltpu.VMEM((rows, cols), BF16),
            pltpu.VMEM((rows, cols), F32),
            pltpu.VMEM((rows, cols), BF16),
            pltpu.VMEM((rows, cols), F32),
            pltpu.VMEM((n_heads, rows, LANES), F32),
            pltpu.VMEM((rows, cols), F32),
            pltpu.VMEM(square, F32),
            pltpu.VMEM((n_heads, 8, LANES), F32),
            pltpu.VMEM(square, BF16),
            pltpu.VMEM(square, BF16),
            pltpu.VMEM((2, rows, cols), BF16),
            pltpu.VMEM((n_fs - 1, 2, rows, cols), BF16),
            pltpu.VMEM((n_fs, rows, out_cols), BF16),
            pltpu.VMEM((n_tp - 1, n_fs, share, out_cols), BF16),
            pltpu.VMEM((n_fs - 1, share, out_cols), BF16),
            pltpu.VMEM((n_fs - 1, share, out_cols), BF16),
            dma((N_PROJ + 2,)),
            dma((n_fs * n_tp,)), dma((n_fs,)),
            dma((n_tp - 1,)), dma((n_tp,)),
            dma(((n_fs - 1) * N_PROJ,)), dma(((n_fs - 1) * N_PROJ,)),
            dma((n_sp * 2,)), dma((n_sp * 2,)),
            dma((2,)),
            dma(((n_fs - 1) * 2,)), dma(((n_fs - 1) * 2,)),
            dma((n_fs * (n_tp - 1),)), dma((n_fs * (n_tp - 1),)),
            dma((n_fs - 1,)), dma((n_fs - 1,)),
        ],
        compiler_params=pltpu.CompilerParams(
            collective_id=0, has_side_effects=True, vmem_limit_bytes=60 * 1024 * 1024
        ),
        name="layer",
    )(
        tokens.reshape(rows, feat_t), mix_gain.reshape(1, width),
        attn_key, attn_value, rec_forget, rec_input, attn_query, rec_query,
        break_offset, forget_room, out_gain.reshape(1, LANES), out_attn, out_rec,
    )
    return result.reshape(1, share, width)


def solution(mesh):
    placed = (
        P(("grp", "fs"), "sp", "tp"),
        P(),
        P("fs", "tp"),
        P("fs", "tp"),
        P("fs", "tp"),
        P("fs", "tp"),
        P("fs", "tp"),
        P("fs", "tp"),
        P("tp"),
        P("tp", None),
        P(),
        P("tp", "fs"),
        P("tp", "fs"),
    )
    return jax.shard_map(
        body,
        mesh=mesh,
        in_specs=placed,
        out_specs=P(("grp", "fs"), ("sp", "tp"), None),
        check_vma=False,
    )
```

```python
import functools
import math

import jax
import jax.numpy as jnp
from jax import lax
from jax.experimental import pallas as pl
from jax.experimental.pallas import tpu as pltpu
from jax.sharding import PartitionSpec as P

LANES = 128
norm_eps = 1e-06
MESH = pl.DeviceIdType.MESH
F32 = jnp.float32
BF16 = jnp.bfloat16
N_PROJ = 6
CHUNKS = 2


def dot_nn(a, b):
    return lax.dot_general(a, b, (((1,), (0,)), ((), ())), preferred_element_type=F32)


def dot_nt(a, b):
    return lax.dot_general(a, b, (((1,), (1,)), ((), ())), preferred_element_type=F32)


def dot_tn(a, b):
    return lax.dot_general(a, b, (((0,), (0,)), ((), ())), preferred_element_type=F32)


def halves(x):
    high = x.astype(BF16)
    return high, (x - high.astype(F32)).astype(BF16)


def kernel(
    n_sp, n_fs, n_tp,
    tok_hbm, gain, w_k, w_v, w_f, w_i, w_q, w_r, offs, room, out_gain, o_attn, o_rec,
    out,
    tok, wbuf, obuf, xt, xg, ss, acc, psend, precv, kv, qbuf, qdec, ecum, kinv,
    att, run, loc, st_loc, dec, st_in, st_out, heads, hrecv, part_acc, part, precv2, mix, mrecv,
    t_sem, w_sem, x_send, x_recv, f_send, ss_send, ss_recv, p_send, p_recv, kv_send, kv_recv,
    st_sem, h_send, h_recv, pp_send, pp_recv, m_send, m_recv,
):
    sp, fs, tp = lax.axis_index("sp"), lax.axis_index("fs"), lax.axis_index("tp")
    rows, feat_t = tok.shape
    feat_f = xt.shape[2]
    width = feat_t * n_tp
    cols = wbuf.shape[2]
    n_heads = cols // LANES
    share = rows // n_tp
    out_cols = obuf.shape[2]
    has_next = sp < n_sp - 1
    has_prev = sp > 0

    def fs_at(step):
        return lax.rem(fs + step, n_fs)

    def tp_at(step):
        return lax.rem(tp + step, n_tp)

    tok_copy = pltpu.make_async_copy(tok_hbm, tok, t_sem.at[0])
    tok_copy.start()
    w_copies = [
        pltpu.make_async_copy(w, wbuf.at[i], w_sem.at[i])
        for i, w in enumerate((w_k, w_v, w_f, w_i, w_q, w_r))
    ]
    w_copies += [
        pltpu.make_async_copy(w, obuf.at[i], w_sem.at[N_PROJ + i])
        for i, w in enumerate((o_attn, o_rec))
    ]
    barrier = pltpu.get_barrier_semaphore()
    for df in range(n_fs):
        for dt in range(n_tp):
            if df or dt:
                pl.semaphore_signal(
                    barrier, inc=1, device_id={"fs": fs_at(df), "tp": tp_at(dt)}, device_id_type=MESH
                )

    @pl.when(has_next)
    def _():
        pl.semaphore_signal(barrier, inc=1, device_id={"sp": sp + 1}, device_id_type=MESH)

    @pl.when(has_prev)
    def _():
        pl.semaphore_signal(barrier, inc=1, device_id={"sp": sp - 1}, device_id_type=MESH)

    for copy in w_copies:
        copy.start()
    tok_copy.wait()

    next_count = jnp.where(has_next, 1, 0)
    prev_count = jnp.where(has_prev, 1, 0)
    pl.semaphore_wait(barrier, n_fs * n_tp - 1 + next_count + prev_count)

    def holder(f_index):
        return (f_index * feat_f) // feat_t

    def x_copy(df, dt):
        dest = fs_at(df)
        start = pl.multiple_of(lax.rem(dest * feat_f, feat_t), LANES)
        part_rows = rows if df == 0 else share
        first = 0 if df == 0 else pl.multiple_of(tp_at(dt) * share, share)
        piece = tp if df == 0 else tp_at(dt)
        return pltpu.make_async_remote_copy(
            src_ref=tok.at[pl.ds(first, part_rows), pl.ds(start, feat_f)],
            dst_ref=xt.at[fs, pl.ds(first, part_rows)],
            send_sem=x_send.at[df * n_tp + dt],
            recv_sem=x_recv.at[fs * n_tp + piece],
            device_id={"fs": dest, "tp": tp_at(dt)},
            device_id_type=MESH,
        )

    def f_copy(df, dt):
        slot = fs_at(df)
        first = pl.multiple_of(tp * share, share)
        return pltpu.make_async_remote_copy(
            src_ref=xt.at[slot, pl.ds(first, share)],
            dst_ref=xt.at[slot, pl.ds(first, share)],
            send_sem=f_send.at[df * n_tp + dt],
            recv_sem=x_recv.at[slot * n_tp + tp],
            device_id={"tp": tp_at(dt)},
            device_id_type=MESH,
        )

    x_order = [(df, dt) for df in list(range(1, n_fs)) + [0] for dt in range(n_tp) if df or dt]
    for df, dt in x_order:
        @pl.when(holder(fs_at(df)) == tp)
        def _(df=df, dt=dt):
            x_copy(df, dt).start()

    squares = jnp.zeros((rows, LANES), F32)
    for c in range(feat_t // LANES):
        piece = tok[:, c * LANES:(c + 1) * LANES].astype(F32)
        squares = squares + piece * piece
    ss[tp] = squares

    def ss_copy(dt):
        return pltpu.make_async_remote_copy(
            src_ref=ss.at[tp], dst_ref=ss.at[tp],
            send_sem=ss_send.at[dt - 1], recv_sem=ss_recv.at[tp],
            device_id={"tp": tp_at(dt)}, device_id_type=MESH,
        )

    for dt in range(1, n_tp):
        ss_copy(dt).start()

    own_holder = holder(fs) == tp
    gain_f = gain[:, pl.ds(pl.multiple_of(fs * feat_f, LANES), feat_f)]

    @pl.when(own_holder)
    def _():
        start = pl.multiple_of(lax.rem(fs * feat_f, feat_t), LANES)
        xg[0] = (tok[:, pl.ds(start, feat_f)].astype(F32) * gain_f).astype(BF16)

    def x_wait(slot, piece, first, count):
        view = xt.at[slot, pl.ds(first, count)]
        pltpu.make_async_remote_copy(
            src_ref=view, dst_ref=view,
            send_sem=x_send.at[0], recv_sem=x_recv.at[slot * n_tp + piece],
            device_id={"tp": tp_at(1)}, device_id_type=MESH,
        ).wait_recv()

    def p_copy(df, w):
        return pltpu.make_async_remote_copy(
            src_ref=psend.at[df - 1, w], dst_ref=precv.at[df - 1, w],
            send_sem=p_send.at[(df - 1) * N_PROJ + w], recv_sem=p_recv.at[(df - 1) * N_PROJ + w],
            device_id={"fs": fs_at(df)}, device_id_type=MESH,
        )

    for df in range(1, n_fs):
        slot = fs_at(df)
        x_wait(slot, tp, pl.multiple_of(tp * share, share), share)
        for dt in range(1, n_tp):
            f_copy(df, dt).start()
    for df in range(1, n_fs):
        slot = fs_at(df)
        for dt in range(1, n_tp):
            piece = tp_at(dt)
            x_wait(slot, piece, pl.multiple_of(piece * share, share), share)
        xg[df] = (xt[slot].astype(F32) * gain_f).astype(BF16)
    for w in range(N_PROJ):
        w_copies[w].wait()
        for df in range(1, n_fs):
            psend[df - 1, w] = dot_nn(xg[df], wbuf[w]).astype(BF16)
            p_copy(df, w).start()

    @pl.when(jnp.logical_not(own_holder))
    def _():
        x_wait(fs, holder(fs), 0, rows)
        xg[0] = (xt[fs].astype(F32) * gain_f).astype(BF16)

    for w in range(N_PROJ):
        acc[w] = dot_nn(xg[0], wbuf[w])

    total = ss[tp]
    for dt in range(1, n_tp):
        other = tp_at(dt)
        pltpu.make_async_remote_copy(
            src_ref=ss.at[other], dst_ref=ss.at[other],
            send_sem=ss_send.at[dt - 1], recv_sem=ss_recv.at[other],
            device_id={"tp": other}, device_id_type=MESH,
        ).wait_recv()
        total = total + ss[other]
    factor = lax.rsqrt(jnp.sum(total, axis=1, keepdims=True) / width + norm_eps)

    def finish(w):
        value = acc[w]
        for df in range(1, n_fs):
            p_copy(df, w).wait_recv()
            value = value + precv[df - 1, w].astype(F32)
        return (value * factor).astype(BF16)

    def kv_copy(slot, c):
        return pltpu.make_async_remote_copy(
            src_ref=kv.at[slot, c], dst_ref=kv.at[slot, c],
            send_sem=kv_send.at[slot * 2 + c], recv_sem=kv_recv.at[slot * 2 + c],
            device_id={"sp": lax.rem(sp + 1, n_sp)}, device_id_type=MESH,
        )

    for c in range(2):
        kv[sp, c] = finish(c)

        @pl.when(has_next)
        def _(c=c):
            kv_copy(sp, c).start()

    def hand_on(step, c):
        kv_copy(sp - step, c).wait_recv()

        @pl.when(has_next)
        def _():
            kv_copy(sp - step, c).start()

    def hand_on_if(step, c):
        if step < n_sp:
            pl.when(sp >= step)(functools.partial(hand_on, step, c))

    hand_on_if(1, 0)
    iota_r = lax.broadcasted_iota(jnp.int32, (rows, rows), 0)
    iota_c = lax.broadcasted_iota(jnp.int32, (rows, rows), 1)
    causal = iota_r >= iota_c
    strict = iota_c < iota_r

    def st_copy(h):
        return pltpu.make_async_remote_copy(
            src_ref=st_out.at[h], dst_ref=st_in.at[h],
            send_sem=st_sem.at[h], recv_sem=st_sem.at[n_heads + h],
            device_id={"sp": lax.rem(sp + 1, n_sp)}, device_id_type=MESH,
        )

    lower = jnp.where(causal, 1.0, 0.0).astype(BF16)
    forget_pre = finish(2)
    hand_on_if(1, 1)
    rec_i = finish(3)
    for h in range(n_heads):
        lanes = slice(h * LANES, (h + 1) * LANES)
        key_in = room[h:h + 1, :] * jax.nn.sigmoid(-forget_pre[:, lanes].astype(F32))
        high, low = halves(jnp.log1p(-key_in))
        cum = dot_nn(lower, high) + dot_nn(lower, low)
        last = cum[rows - 1:rows, :]
        ecum[:, lanes] = jnp.exp(cum)
        kinv[:, lanes] = (key_in * jnp.exp(-cum)).astype(BF16)
        fresh = (key_in * jnp.exp(last - cum)).astype(BF16)
        st_loc[h] = dot_tn(rec_i[:, lanes], fresh)
        dec[h] = jnp.broadcast_to(jnp.exp(last), dec.shape[1:])

        @pl.when(jnp.logical_and(sp == 0, has_next))
        def _(h=h):
            st_out[h] = st_loc[h].astype(BF16)
            st_copy(h).start()

    hand_on_if(2, 0)

    qbuf[...] = finish(4)
    later = jnp.where(iota_r > iota_c, 1.0, 0.0).astype(BF16)
    sums = jnp.concatenate([later, jnp.ones((rows, LANES), BF16)], axis=1)
    scale = 1.0 / math.sqrt(LANES)

    def attend(slot, diagonal):
        for h in range(n_heads):
            lanes = slice(h * LANES, (h + 1) * LANES)
            z = dot_nt(qbuf[:, lanes], kv[slot, 0, :, lanes]) * scale + offs[h]
            keep = -(jnp.maximum(z, 0.0) + jnp.log1p(jnp.exp(-jnp.abs(z))))
            log_stick = z + keep
            if diagonal:
                keep = jnp.where(strict, keep, 0.0)
            high, low = halves(keep)
            both = dot_nn(high, sums) + dot_nn(low, sums)
            stick = jnp.exp(log_stick + both[:, :rows])
            if diagonal:
                stick = jnp.where(strict, stick, 0.0)
            value = dot_nn(stick.astype(BF16), kv[slot, 1, :, lanes])
            if diagonal:
                att[:, lanes] = value
                run[h] = both[:, rows:]
            else:
                past = run[h]
                att[:, lanes] += value * jnp.exp(past)
                run[h] = past + both[:, rows:]

    def attend_if(step):
        if step < n_sp:
            @pl.when(sp >= step)
            def _():
                attend(sp - step, False)

    attend(sp, True)
    attend_if(1)
    hand_on_if(2, 1)
    rec_q = finish(5)
    for h in range(n_heads):
        lanes = slice(h * LANES, (h + 1) * LANES)
        decayed = (rec_q[:, lanes].astype(F32) * ecum[:, lanes]).astype(BF16)
        qdec[:, lanes] = decayed
        scores = jnp.where(causal, dot_nt(decayed, kinv[:, lanes]), 0.0)
        loc[:, lanes] = dot_nn(scores.astype(BF16), rec_i[:, lanes])

    attend_if(2)

    def block(step, carry):
        for c in range(2):
            hand_on(step, c)
        attend(sp - step, False)
        return carry

    lax.fori_loop(3, sp + 1, block, 0)

    def h_copy(df, c):
        index = (df - 1) * (1 + n_heads) + c
        if c == 0:
            source, target = heads.at[0], hrecv.at[df - 1, 0]
        else:
            lanes = pl.ds((c - 1) * LANES, LANES)
            source, target = heads.at[1, :, lanes], hrecv.at[df - 1, 1, :, lanes]
        return pltpu.make_async_remote_copy(
            src_ref=source, dst_ref=target, send_sem=h_send.at[index], recv_sem=h_recv.at[index],
            device_id={"fs": fs_at(df)}, device_id_type=MESH,
        )

    heads[0] = att[...].astype(BF16)
    for df in range(1, n_fs):
        h_copy(df, 0).start()

    for h in range(n_heads):
        lanes = slice(h * LANES, (h + 1) * LANES)

        @pl.when(has_prev)
        def _(h=h, lanes=lanes):
            st_copy(h).wait_recv()

            @pl.when(has_next)
            def _():
                st_out[h] = (st_in[h].astype(F32) * dec[h, 0:1, :] + st_loc[h]).astype(BF16)
                st_copy(h).start()

            loc[:, lanes] += dot_nt(qdec[:, lanes], st_in[h])

        raw = loc[:, lanes]
        norm = lax.rsqrt(jnp.mean(raw * raw, axis=1, keepdims=True) + norm_eps)
        heads[1, :, lanes] = (raw * norm * out_gain[...]).astype(BF16)
        for df in range(1, n_fs):
            h_copy(df, 1 + h).start()

    w_copies[N_PROJ].wait()
    w_copies[N_PROJ + 1].wait()

    half = out_cols // CHUNKS

    def pp_copy(df, dt, k):
        index = (df * (n_tp - 1) + dt - 1) * CHUNKS + k
        start = pl.multiple_of(tp_at(dt) * share, share)
        return pltpu.make_async_remote_copy(
            src_ref=part.at[df, k, pl.ds(start, share)], dst_ref=precv2.at[dt - 1, df, k],
            send_sem=pp_send.at[index], recv_sem=pp_recv.at[index],
            device_id={"tp": tp_at(dt)}, device_id_type=MESH,
        )

    def m_copy(df, k):
        index = (df - 1) * CHUNKS + k
        return pltpu.make_async_remote_copy(
            src_ref=mix.at[df - 1, k], dst_ref=mrecv.at[df - 1, k],
            send_sem=m_send.at[index], recv_sem=m_recv.at[index],
            device_id={"fs": fs_at(df)}, device_id_type=MESH,
        )

    def reduced(df, k):
        value = part[df, k, pl.ds(pl.multiple_of(tp * share, share), share)].astype(F32)
        for dt in range(1, n_tp):
            pp_copy(df, dt, k).wait_recv()
            value = value + precv2[dt - 1, df, k].astype(F32)
        return value.astype(BF16)

    def columns(owner, k):
        return pl.ds(pl.multiple_of(owner * out_cols + k * half, LANES), half)

    for df in range(1, n_fs):
        h_copy(df, 0).wait_recv()
        for k in range(CHUNKS):
            part_acc[df - 1, k] = dot_nn(hrecv[df - 1, 0], obuf[0, :, k * half:(k + 1) * half])
    for k in range(CHUNKS):
        cut = slice(k * half, (k + 1) * half)
        part[0, k] = (dot_nn(heads[0], obuf[0, :, cut]) + dot_nn(heads[1], obuf[1, :, cut])).astype(BF16)
        for dt in range(1, n_tp):
            pp_copy(0, dt, k).start()
    for df in range(1, n_fs):
        for h in range(n_heads):
            h_copy(df, 1 + h).wait_recv()
        for k in range(CHUNKS):
            cut = slice(k * half, (k + 1) * half)
            part[df, k] = (part_acc[df - 1, k] + dot_nn(hrecv[df - 1, 1], obuf[1, :, cut])).astype(BF16)
            for dt in range(1, n_tp):
                pp_copy(df, dt, k).start()
    for df in range(1, n_fs):
        for k in range(CHUNKS):
            mix[df - 1, k] = reduced(df, k)
            m_copy(df, k).start()
    for k in range(CHUNKS):
        out[:, columns(fs, k)] = reduced(0, k)
    for df in range(1, n_fs):
        source = lax.rem(fs + n_fs - df, n_fs)
        for k in range(CHUNKS):
            m_copy(df, k).wait_recv()
            out[:, columns(source, k)] = mrecv[df - 1, k]

    for df, dt in x_order:
        @pl.when(holder(fs_at(df)) == tp)
        def _(df=df, dt=dt):
            x_copy(df, dt).wait_send()
    for dt in range(1, n_tp):
        ss_copy(dt).wait_send()
        for df in range(1, n_fs):
            f_copy(df, dt).wait_send()
    for df in range(1, n_fs):
        for w in range(N_PROJ):
            p_copy(df, w).wait_send()
        for c in range(1 + n_heads):
            h_copy(df, c).wait_send()
    for k in range(CHUNKS):
        for df in range(1, n_fs):
            m_copy(df, k).wait_send()
        for df in range(n_fs):
            for dt in range(1, n_tp):
                pp_copy(df, dt, k).wait_send()

    @pl.when(has_next)
    def _():
        for h in range(n_heads):
            st_copy(h).wait_send()

        def drain(slot, carry):
            for c in range(2):
                kv_copy(slot, c).wait_send()
            return carry

        lax.fori_loop(0, sp + 1, drain, 0)


def body(
    tokens, mix_gain, attn_query, attn_key, attn_value, rec_query, rec_forget, rec_input,
    break_offset, forget_room, out_gain, out_attn, out_rec,
):
    n_sp, n_fs, n_tp = lax.axis_size("sp"), lax.axis_size("fs"), lax.axis_size("tp")
    rows, feat_t = tokens.shape[1], tokens.shape[2]
    feat_f, cols = attn_query.shape
    width = feat_t * n_tp
    n_heads = cols // LANES
    out_rows, out_cols = out_attn.shape
    share = rows // n_tp
    piece = out_cols // CHUNKS
    vmem = pl.BlockSpec(memory_space=pltpu.VMEM)
    smem = pl.BlockSpec(memory_space=pltpu.SMEM)
    hbm = pl.BlockSpec(memory_space=pl.ANY)
    dma = pltpu.SemaphoreType.DMA
    square = (n_heads, LANES, LANES)
    result = pl.pallas_call(
        functools.partial(kernel, n_sp, n_fs, n_tp),
        out_shape=jax.ShapeDtypeStruct((share, width), BF16),
        in_specs=[hbm, vmem] + [hbm] * 6 + [smem, vmem, vmem, hbm, hbm],
        out_specs=vmem,
        scratch_shapes=[
            pltpu.VMEM((rows, feat_t), BF16),
            pltpu.VMEM((N_PROJ, feat_f, cols), BF16),
            pltpu.VMEM((2, out_rows, out_cols), BF16),
            pltpu.VMEM((n_fs, rows, feat_f), BF16),
            pltpu.VMEM((n_fs, rows, feat_f), BF16),
            pltpu.VMEM((n_tp, rows, LANES), F32),
            pltpu.VMEM((N_PROJ, rows, cols), F32),
            pltpu.VMEM((n_fs - 1, N_PROJ, rows, cols), BF16),
            pltpu.VMEM((n_fs - 1, N_PROJ, rows, cols), BF16),
            pltpu.VMEM((n_sp, 2, rows, cols), BF16),
            pltpu.VMEM((rows, cols), BF16),
            pltpu.VMEM((rows, cols), BF16),
            pltpu.VMEM((rows, cols), F32),
            pltpu.VMEM((rows, cols), BF16),
            pltpu.VMEM((rows, cols), F32),
            pltpu.VMEM((n_heads, rows, LANES), F32),
            pltpu.VMEM((rows, cols), F32),
            pltpu.VMEM(square, F32),
            pltpu.VMEM((n_heads, 8, LANES), F32),
            pltpu.VMEM(square, BF16),
            pltpu.VMEM(square, BF16),
            pltpu.VMEM((2, rows, cols), BF16),
            pltpu.VMEM((n_fs - 1, 2, rows, cols), BF16),
            pltpu.VMEM((n_fs - 1, CHUNKS, rows, piece), F32),
            pltpu.VMEM((n_fs, CHUNKS, rows, piece), BF16),
            pltpu.VMEM((n_tp - 1, n_fs, CHUNKS, share, piece), BF16),
            pltpu.VMEM((n_fs - 1, CHUNKS, share, piece), BF16),
            pltpu.VMEM((n_fs - 1, CHUNKS, share, piece), BF16),
            dma((1,)), dma((N_PROJ + 2,)),
            dma((n_fs * n_tp,)), dma((n_fs * n_tp,)), dma((n_fs * n_tp,)),
            dma((n_tp - 1,)), dma((n_tp,)),
            dma(((n_fs - 1) * N_PROJ,)), dma(((n_fs - 1) * N_PROJ,)),
            dma((n_sp * 2,)), dma((n_sp * 2,)),
            dma((2 * n_heads,)),
            dma(((n_fs - 1) * (1 + n_heads),)), dma(((n_fs - 1) * (1 + n_heads),)),
            dma((n_fs * (n_tp - 1) * CHUNKS,)), dma((n_fs * (n_tp - 1) * CHUNKS,)),
            dma(((n_fs - 1) * CHUNKS,)), dma(((n_fs - 1) * CHUNKS,)),
        ],
        compiler_params=pltpu.CompilerParams(
            collective_id=0, has_side_effects=True, vmem_limit_bytes=60 * 1024 * 1024
        ),
        name="layer",
    )(
        tokens.reshape(rows, feat_t), mix_gain.reshape(1, width),
        attn_key, attn_value, rec_forget, rec_input, attn_query, rec_query,
        break_offset, forget_room, out_gain.reshape(1, LANES), out_attn, out_rec,
    )
    return result.reshape(1, share, width)


def solution(mesh):
    placed = (
        P(("grp", "fs"), "sp", "tp"),
        P(),
        P("fs", "tp"),
        P("fs", "tp"),
        P("fs", "tp"),
        P("fs", "tp"),
        P("fs", "tp"),
        P("fs", "tp"),
        P("tp"),
        P("tp", None),
        P(),
        P("tp", "fs"),
        P("tp", "fs"),
    )
    return jax.shard_map(
        body,
        mesh=mesh,
        in_specs=placed,
        out_specs=P(("grp", "fs"), ("sp", "tp"), None),
        check_vma=False,
    )
```

```python
import functools
import math

import jax
import jax.numpy as jnp
from jax import lax
from jax.experimental import pallas as pl
from jax.experimental.pallas import tpu as pltpu
from jax.sharding import PartitionSpec as P

LANES = 128
norm_eps = 1e-06
MESH = pl.DeviceIdType.MESH
F32 = jnp.float32
BF16 = jnp.bfloat16
N_PROJ = 6
GROUPS = 2
CHUNKS = 2


def dot_nn(a, b):
    return lax.dot_general(a, b, (((1,), (0,)), ((), ())), preferred_element_type=F32)


def dot_nt(a, b):
    return lax.dot_general(a, b, (((1,), (1,)), ((), ())), preferred_element_type=F32)


def dot_tn(a, b):
    return lax.dot_general(a, b, (((0,), (0,)), ((), ())), preferred_element_type=F32)


def halves(x):
    high = x.astype(BF16)
    return high, (x - high.astype(F32)).astype(BF16)


def kernel(
    n_sp, n_fs, n_tp,
    tok_hbm, gain, w_k, w_v, w_f, w_i, w_q, w_r, offs, room, out_gain, o_attn, o_rec,
    out,
    tok, wbuf, obuf, xt, xg, ss, acc, psend, precv, kv, qbuf, qdec, ecum, kinv,
    att, run, loc, st_loc, dec, st_in, st_out, heads, hrecv, part_acc, part, precv2, mix, mrecv,
    t_sem, w_sem, x_send, x_recv, f_send, ss_send, ss_recv, p_send, p_recv, kv_send, kv_recv,
    st_sem, h_send, h_recv, pp_send, pp_recv, m_send, m_recv,
):
    sp, fs, tp = lax.axis_index("sp"), lax.axis_index("fs"), lax.axis_index("tp")
    rows, feat_t = tok.shape
    feat_f = xt.shape[2]
    width = feat_t * n_tp
    cols = wbuf.shape[2]
    n_heads = cols // LANES
    share = rows // n_tp
    out_cols = obuf.shape[2]
    has_next = sp < n_sp - 1
    has_prev = sp > 0

    def fs_at(step):
        return lax.rem(fs + step, n_fs)

    def tp_at(step):
        return lax.rem(tp + step, n_tp)

    tok_copy = pltpu.make_async_copy(tok_hbm, tok, t_sem.at[0])
    tok_copy.start()
    w_copies = [
        pltpu.make_async_copy(w, wbuf.at[i], w_sem.at[i])
        for i, w in enumerate((w_k, w_v, w_f, w_i, w_q, w_r))
    ]
    w_copies += [
        pltpu.make_async_copy(w, obuf.at[i], w_sem.at[N_PROJ + i])
        for i, w in enumerate((o_attn, o_rec))
    ]
    barrier = pltpu.get_barrier_semaphore()
    for df in range(n_fs):
        for dt in range(n_tp):
            if df or dt:
                pl.semaphore_signal(
                    barrier, inc=1, device_id={"fs": fs_at(df), "tp": tp_at(dt)}, device_id_type=MESH
                )

    @pl.when(has_next)
    def _():
        pl.semaphore_signal(barrier, inc=1, device_id={"sp": sp + 1}, device_id_type=MESH)

    @pl.when(has_prev)
    def _():
        pl.semaphore_signal(barrier, inc=1, device_id={"sp": sp - 1}, device_id_type=MESH)

    for copy in w_copies:
        copy.start()
    tok_copy.wait()

    next_count = jnp.where(has_next, 1, 0)
    prev_count = jnp.where(has_prev, 1, 0)
    pl.semaphore_wait(barrier, n_fs * n_tp - 1 + next_count + prev_count)

    def holder(f_index):
        return (f_index * feat_f) // feat_t

    def x_copy(df, dt):
        dest = fs_at(df)
        start = pl.multiple_of(lax.rem(dest * feat_f, feat_t), LANES)
        part_rows = rows if df == 0 else share
        first = 0 if df == 0 else pl.multiple_of(tp_at(dt) * share, share)
        piece = tp if df == 0 else tp_at(dt)
        return pltpu.make_async_remote_copy(
            src_ref=tok.at[pl.ds(first, part_rows), pl.ds(start, feat_f)],
            dst_ref=xt.at[fs, pl.ds(first, part_rows)],
            send_sem=x_send.at[df * n_tp + dt],
            recv_sem=x_recv.at[fs * n_tp + piece],
            device_id={"fs": dest, "tp": tp_at(dt)},
            device_id_type=MESH,
        )

    def f_copy(df, dt):
        slot = fs_at(df)
        first = pl.multiple_of(tp * share, share)
        return pltpu.make_async_remote_copy(
            src_ref=xt.at[slot, pl.ds(first, share)],
            dst_ref=xt.at[slot, pl.ds(first, share)],
            send_sem=f_send.at[df * n_tp + dt],
            recv_sem=x_recv.at[slot * n_tp + tp],
            device_id={"tp": tp_at(dt)},
            device_id_type=MESH,
        )

    x_order = [(df, dt) for df in list(range(1, n_fs)) + [0] for dt in range(n_tp) if df or dt]
    for df, dt in x_order:
        @pl.when(holder(fs_at(df)) == tp)
        def _(df=df, dt=dt):
            x_copy(df, dt).start()

    squares = jnp.zeros((rows, LANES), F32)
    for c in range(feat_t // LANES):
        piece = tok[:, c * LANES:(c + 1) * LANES].astype(F32)
        squares = squares + piece * piece
    ss[tp] = squares

    def ss_copy(dt):
        return pltpu.make_async_remote_copy(
            src_ref=ss.at[tp], dst_ref=ss.at[tp],
            send_sem=ss_send.at[dt - 1], recv_sem=ss_recv.at[tp],
            device_id={"tp": tp_at(dt)}, device_id_type=MESH,
        )

    for dt in range(1, n_tp):
        ss_copy(dt).start()

    own_holder = holder(fs) == tp
    gain_f = gain[:, pl.ds(pl.multiple_of(fs * feat_f, LANES), feat_f)]

    @pl.when(own_holder)
    def _():
        start = pl.multiple_of(lax.rem(fs * feat_f, feat_t), LANES)
        xg[0] = (tok[:, pl.ds(start, feat_f)].astype(F32) * gain_f).astype(BF16)

    def x_wait(slot, piece, first, count):
        view = xt.at[slot, pl.ds(first, count)]
        pltpu.make_async_remote_copy(
            src_ref=view, dst_ref=view,
            send_sem=x_send.at[0], recv_sem=x_recv.at[slot * n_tp + piece],
            device_id={"tp": tp_at(1)}, device_id_type=MESH,
        ).wait_recv()

    g_cols = cols // GROUPS
    units = [(w, g * g_cols, g_cols) for g in range(GROUPS) for w in (0, 1)]
    units += [(w, 0, cols) for w in range(2, N_PROJ)]
    n_units = len(units)
    n_kv = 2 * GROUPS

    def p_copy(df, u):
        w, first, count = units[u]
        return pltpu.make_async_remote_copy(
            src_ref=psend.at[df - 1, w, :, pl.ds(first, count)],
            dst_ref=precv.at[df - 1, w, :, pl.ds(first, count)],
            send_sem=p_send.at[(df - 1) * n_units + u], recv_sem=p_recv.at[(df - 1) * n_units + u],
            device_id={"fs": fs_at(df)}, device_id_type=MESH,
        )

    for df in range(1, n_fs):
        slot = fs_at(df)
        x_wait(slot, tp, pl.multiple_of(tp * share, share), share)
        for dt in range(1, n_tp):
            f_copy(df, dt).start()
    for df in range(1, n_fs):
        slot = fs_at(df)
        for dt in range(1, n_tp):
            piece = tp_at(dt)
            x_wait(slot, piece, pl.multiple_of(piece * share, share), share)
        xg[df] = (xt[slot].astype(F32) * gain_f).astype(BF16)
    for u, (w, first, count) in enumerate(units):
        if first == 0:
            w_copies[w].wait()
        cut = slice(first, first + count)
        for df in range(1, n_fs):
            psend[df - 1, w, :, cut] = dot_nn(xg[df], wbuf[w, :, cut]).astype(BF16)
            p_copy(df, u).start()

    @pl.when(jnp.logical_not(own_holder))
    def _():
        x_wait(fs, holder(fs), 0, rows)
        xg[0] = (xt[fs].astype(F32) * gain_f).astype(BF16)

    for w in range(N_PROJ):
        acc[w] = dot_nn(xg[0], wbuf[w])

    total = ss[tp]
    for dt in range(1, n_tp):
        other = tp_at(dt)
        pltpu.make_async_remote_copy(
            src_ref=ss.at[other], dst_ref=ss.at[other],
            send_sem=ss_send.at[dt - 1], recv_sem=ss_recv.at[other],
            device_id={"tp": other}, device_id_type=MESH,
        ).wait_recv()
        total = total + ss[other]
    factor = lax.rsqrt(jnp.sum(total, axis=1, keepdims=True) / width + norm_eps)

    def finish(u):
        w, first, count = units[u]
        cut = slice(first, first + count)
        value = acc[w, :, cut]
        for df in range(1, n_fs):
            p_copy(df, u).wait_recv()
            value = value + precv[df - 1, w, :, cut].astype(F32)
        return (value * factor).astype(BF16)

    def kv_copy(slot, c):
        return pltpu.make_async_remote_copy(
            src_ref=kv.at[slot, c], dst_ref=kv.at[slot, c],
            send_sem=kv_send.at[slot * n_kv + c], recv_sem=kv_recv.at[slot * n_kv + c],
            device_id={"sp": lax.rem(sp + 1, n_sp)}, device_id_type=MESH,
        )

    for c in range(n_kv):
        kv[sp, c] = finish(c)

        @pl.when(has_next)
        def _(c=c):
            kv_copy(sp, c).start()

    def hand_on(step, c):
        kv_copy(sp - step, c).wait_recv()

        @pl.when(has_next)
        def _():
            kv_copy(sp - step, c).start()

    def hand_on_if(step, c):
        if step < n_sp:
            pl.when(sp >= step)(functools.partial(hand_on, step, c))

    hand_on_if(1, 0)
    hand_on_if(1, 1)
    iota_r = lax.broadcasted_iota(jnp.int32, (rows, rows), 0)
    iota_c = lax.broadcasted_iota(jnp.int32, (rows, rows), 1)
    causal = iota_r >= iota_c
    strict = iota_c < iota_r

    def st_copy(h):
        return pltpu.make_async_remote_copy(
            src_ref=st_out.at[h], dst_ref=st_in.at[h],
            send_sem=st_sem.at[h], recv_sem=st_sem.at[n_heads + h],
            device_id={"sp": lax.rem(sp + 1, n_sp)}, device_id_type=MESH,
        )

    lower = jnp.where(causal, 1.0, 0.0).astype(BF16)
    forget_pre = finish(n_kv)
    for c in range(2, n_kv):
        hand_on_if(1, c)
    rec_i = finish(n_kv + 1)
    for h in range(n_heads):
        lanes = slice(h * LANES, (h + 1) * LANES)
        key_in = room[h:h + 1, :] * jax.nn.sigmoid(-forget_pre[:, lanes].astype(F32))
        high, low = halves(jnp.log1p(-key_in))
        cum = dot_nn(lower, high) + dot_nn(lower, low)
        last = cum[rows - 1:rows, :]
        ecum[:, lanes] = jnp.exp(cum)
        kinv[:, lanes] = (key_in * jnp.exp(-cum)).astype(BF16)
        fresh = (key_in * jnp.exp(last - cum)).astype(BF16)
        st_loc[h] = dot_tn(rec_i[:, lanes], fresh)
        dec[h] = jnp.broadcast_to(jnp.exp(last), dec.shape[1:])

        @pl.when(jnp.logical_and(sp == 0, has_next))
        def _(h=h):
            st_out[h] = st_loc[h].astype(BF16)
            st_copy(h).start()

    hand_on_if(2, 0)
    hand_on_if(2, 1)

    qbuf[...] = finish(n_kv + 2)
    later = jnp.where(iota_r > iota_c, 1.0, 0.0).astype(BF16)
    sums = jnp.concatenate([later, jnp.ones((rows, LANES), BF16)], axis=1)
    scale = 1.0 / math.sqrt(LANES)

    g_heads = n_heads // GROUPS

    def attend(slot, g, diagonal):
        for h in range(g * g_heads, (g + 1) * g_heads):
            lanes = slice(h * LANES, (h + 1) * LANES)
            inner = slice((h - g * g_heads) * LANES, (h - g * g_heads + 1) * LANES)
            z = dot_nt(qbuf[:, lanes], kv[slot, 2 * g, :, inner]) * scale + offs[h]
            keep = -(jnp.maximum(z, 0.0) + jnp.log1p(jnp.exp(-jnp.abs(z))))
            log_stick = z + keep
            if diagonal:
                keep = jnp.where(strict, keep, 0.0)
            high, low = halves(keep)
            both = dot_nn(high, sums) + dot_nn(low, sums)
            stick = jnp.exp(log_stick + both[:, :rows])
            if diagonal:
                stick = jnp.where(strict, stick, 0.0)
            value = dot_nn(stick.astype(BF16), kv[slot, 2 * g + 1, :, inner])
            if diagonal:
                att[:, lanes] = value
                run[h] = both[:, rows:]
            else:
                past = run[h]
                att[:, lanes] += value * jnp.exp(past)
                run[h] = past + both[:, rows:]

    def attend_if(step):
        if step < n_sp:
            @pl.when(sp >= step)
            def _():
                for g in range(GROUPS):
                    attend(sp - step, g, False)

    for g in range(GROUPS):
        attend(sp, g, True)
    for c in range(2, n_kv):
        hand_on_if(2, c)
    attend_if(1)
    rec_q = finish(n_kv + 3)
    for h in range(n_heads):
        lanes = slice(h * LANES, (h + 1) * LANES)
        decayed = (rec_q[:, lanes].astype(F32) * ecum[:, lanes]).astype(BF16)
        qdec[:, lanes] = decayed
        scores = jnp.where(causal, dot_nt(decayed, kinv[:, lanes]), 0.0)
        loc[:, lanes] = dot_nn(scores.astype(BF16), rec_i[:, lanes])

    attend_if(2)

    def block(step, carry):
        for c in range(n_kv):
            hand_on(step, c)
        for g in range(GROUPS):
            attend(sp - step, g, False)
        return carry

    lax.fori_loop(3, sp, block, 0)

    n_head_units = GROUPS + n_heads

    def h_copy(df, c):
        index = (df - 1) * n_head_units + c
        if c < GROUPS:
            lanes = pl.ds(c * g_cols, g_cols)
            source, target = heads.at[0, :, lanes], hrecv.at[df - 1, 0, :, lanes]
        else:
            lanes = pl.ds((c - GROUPS) * LANES, LANES)
            source, target = heads.at[1, :, lanes], hrecv.at[df - 1, 1, :, lanes]
        return pltpu.make_async_remote_copy(
            src_ref=source, dst_ref=target, send_sem=h_send.at[index], recv_sem=h_recv.at[index],
            device_id={"fs": fs_at(df)}, device_id_type=MESH,
        )

    for g in range(GROUPS):
        @pl.when(sp >= 3)
        def _(g=g):
            for c in (2 * g, 2 * g + 1):
                hand_on(sp, c)
            attend(0, g, False)

        cut = slice(g * g_cols, (g + 1) * g_cols)
        heads[0, :, cut] = att[:, cut].astype(BF16)
        for df in range(1, n_fs):
            h_copy(df, g).start()

    for h in range(n_heads):
        lanes = slice(h * LANES, (h + 1) * LANES)

        @pl.when(has_prev)
        def _(h=h, lanes=lanes):
            st_copy(h).wait_recv()

            @pl.when(has_next)
            def _():
                st_out[h] = (st_in[h].astype(F32) * dec[h, 0:1, :] + st_loc[h]).astype(BF16)
                st_copy(h).start()

            loc[:, lanes] += dot_nt(qdec[:, lanes], st_in[h])

        raw = loc[:, lanes]
        norm = lax.rsqrt(jnp.mean(raw * raw, axis=1, keepdims=True) + norm_eps)
        heads[1, :, lanes] = (raw * norm * out_gain[...]).astype(BF16)
        for df in range(1, n_fs):
            h_copy(df, GROUPS + h).start()

    w_copies[N_PROJ].wait()
    w_copies[N_PROJ + 1].wait()

    half = out_cols // CHUNKS

    def pp_copy(df, dt, k):
        index = (df * (n_tp - 1) + dt - 1) * CHUNKS + k
        start = pl.multiple_of(tp_at(dt) * share, share)
        return pltpu.make_async_remote_copy(
            src_ref=part.at[df, k, pl.ds(start, share)], dst_ref=precv2.at[dt - 1, df, k],
            send_sem=pp_send.at[index], recv_sem=pp_recv.at[index],
            device_id={"tp": tp_at(dt)}, device_id_type=MESH,
        )

    def m_copy(df, k):
        index = (df - 1) * CHUNKS + k
        return pltpu.make_async_remote_copy(
            src_ref=mix.at[df - 1, k], dst_ref=mrecv.at[df - 1, k],
            send_sem=m_send.at[index], recv_sem=m_recv.at[index],
            device_id={"fs": fs_at(df)}, device_id_type=MESH,
        )

    def reduced(df, k):
        value = part[df, k, pl.ds(pl.multiple_of(tp * share, share), share)].astype(F32)
        for dt in range(1, n_tp):
            pp_copy(df, dt, k).wait_recv()
            value = value + precv2[dt - 1, df, k].astype(F32)
        return value.astype(BF16)

    def columns(owner, k):
        return pl.ds(pl.multiple_of(owner * out_cols + k * half, LANES), half)

    for df in range(1, n_fs):
        for g in range(GROUPS):
            h_copy(df, g).wait_recv()
        for k in range(CHUNKS):
            part_acc[df - 1, k] = dot_nn(hrecv[df - 1, 0], obuf[0, :, k * half:(k + 1) * half])
    for k in range(CHUNKS):
        cut = slice(k * half, (k + 1) * half)
        part[0, k] = (dot_nn(heads[0], obuf[0, :, cut]) + dot_nn(heads[1], obuf[1, :, cut])).astype(BF16)
        for dt in range(1, n_tp):
            pp_copy(0, dt, k).start()
    for df in range(1, n_fs):
        for h in range(n_heads):
            h_copy(df, GROUPS + h).wait_recv()
        for k in range(CHUNKS):
            cut = slice(k * half, (k + 1) * half)
            part[df, k] = (part_acc[df - 1, k] + dot_nn(hrecv[df - 1, 1], obuf[1, :, cut])).astype(BF16)
            for dt in range(1, n_tp):
                pp_copy(df, dt, k).start()
    for df in range(1, n_fs):
        for k in range(CHUNKS):
            mix[df - 1, k] = reduced(df, k)
            m_copy(df, k).start()
    for k in range(CHUNKS):
        out[:, columns(fs, k)] = reduced(0, k)
    for df in range(1, n_fs):
        source = lax.rem(fs + n_fs - df, n_fs)
        for k in range(CHUNKS):
            m_copy(df, k).wait_recv()
            out[:, columns(source, k)] = mrecv[df - 1, k]

    for df, dt in x_order:
        @pl.when(holder(fs_at(df)) == tp)
        def _(df=df, dt=dt):
            x_copy(df, dt).wait_send()
    for dt in range(1, n_tp):
        ss_copy(dt).wait_send()
        for df in range(1, n_fs):
            f_copy(df, dt).wait_send()
    for df in range(1, n_fs):
        for u in range(n_units):
            p_copy(df, u).wait_send()
        for c in range(n_head_units):
            h_copy(df, c).wait_send()
    for k in range(CHUNKS):
        for df in range(1, n_fs):
            m_copy(df, k).wait_send()
        for df in range(n_fs):
            for dt in range(1, n_tp):
                pp_copy(df, dt, k).wait_send()

    @pl.when(has_next)
    def _():
        for h in range(n_heads):
            st_copy(h).wait_send()

        def drain(slot, carry):
            for c in range(n_kv):
                kv_copy(slot, c).wait_send()
            return carry

        lax.fori_loop(0, sp + 1, drain, 0)


def body(
    tokens, mix_gain, attn_query, attn_key, attn_value, rec_query, rec_forget, rec_input,
    break_offset, forget_room, out_gain, out_attn, out_rec,
):
    n_sp, n_fs, n_tp = lax.axis_size("sp"), lax.axis_size("fs"), lax.axis_size("tp")
    rows, feat_t = tokens.shape[1], tokens.shape[2]
    feat_f, cols = attn_query.shape
    width = feat_t * n_tp
    n_heads = cols // LANES
    out_rows, out_cols = out_attn.shape
    share = rows // n_tp
    piece = out_cols // CHUNKS
    n_units = 2 * GROUPS + N_PROJ - 2
    vmem = pl.BlockSpec(memory_space=pltpu.VMEM)
    smem = pl.BlockSpec(memory_space=pltpu.SMEM)
    hbm = pl.BlockSpec(memory_space=pl.ANY)
    dma = pltpu.SemaphoreType.DMA
    square = (n_heads, LANES, LANES)
    result = pl.pallas_call(
        functools.partial(kernel, n_sp, n_fs, n_tp),
        out_shape=jax.ShapeDtypeStruct((share, width), BF16),
        in_specs=[hbm, vmem] + [hbm] * 6 + [smem, vmem, vmem, hbm, hbm],
        out_specs=vmem,
        scratch_shapes=[
            pltpu.VMEM((rows, feat_t), BF16),
            pltpu.VMEM((N_PROJ, feat_f, cols), BF16),
            pltpu.VMEM((2, out_rows, out_cols), BF16),
            pltpu.VMEM((n_fs, rows, feat_f), BF16),
            pltpu.VMEM((n_fs, rows, feat_f), BF16),
            pltpu.VMEM((n_tp, rows, LANES), F32),
            pltpu.VMEM((N_PROJ, rows, cols), F32),
            pltpu.VMEM((n_fs - 1, N_PROJ, rows, cols), BF16),
            pltpu.VMEM((n_fs - 1, N_PROJ, rows, cols), BF16),
            pltpu.VMEM((n_sp, 2 * GROUPS, rows, cols // GROUPS), BF16),
            pltpu.VMEM((rows, cols), BF16),
            pltpu.VMEM((rows, cols), BF16),
            pltpu.VMEM((rows, cols), F32),
            pltpu.VMEM((rows, cols), BF16),
            pltpu.VMEM((rows, cols), F32),
            pltpu.VMEM((n_heads, rows, LANES), F32),
            pltpu.VMEM((rows, cols), F32),
            pltpu.VMEM(square, F32),
            pltpu.VMEM((n_heads, 8, LANES), F32),
            pltpu.VMEM(square, BF16),
            pltpu.VMEM(square, BF16),
            pltpu.VMEM((2, rows, cols), BF16),
            pltpu.VMEM((n_fs - 1, 2, rows, cols), BF16),
            pltpu.VMEM((n_fs - 1, CHUNKS, rows, piece), F32),
            pltpu.VMEM((n_fs, CHUNKS, rows, piece), BF16),
            pltpu.VMEM((n_tp - 1, n_fs, CHUNKS, share, piece), BF16),
            pltpu.VMEM((n_fs - 1, CHUNKS, share, piece), BF16),
            pltpu.VMEM((n_fs - 1, CHUNKS, share, piece), BF16),
            dma((1,)), dma((N_PROJ + 2,)),
            dma((n_fs * n_tp,)), dma((n_fs * n_tp,)), dma((n_fs * n_tp,)),
            dma((n_tp - 1,)), dma((n_tp,)),
            dma(((n_fs - 1) * n_units,)), dma(((n_fs - 1) * n_units,)),
            dma((n_sp * 2 * GROUPS,)), dma((n_sp * 2 * GROUPS,)),
            dma((2 * n_heads,)),
            dma(((n_fs - 1) * (GROUPS + n_heads),)), dma(((n_fs - 1) * (GROUPS + n_heads),)),
            dma((n_fs * (n_tp - 1) * CHUNKS,)), dma((n_fs * (n_tp - 1) * CHUNKS,)),
            dma(((n_fs - 1) * CHUNKS,)), dma(((n_fs - 1) * CHUNKS,)),
        ],
        compiler_params=pltpu.CompilerParams(
            collective_id=0, has_side_effects=True, vmem_limit_bytes=60 * 1024 * 1024
        ),
        name="layer",
    )(
        tokens.reshape(rows, feat_t), mix_gain.reshape(1, width),
        attn_key, attn_value, rec_forget, rec_input, attn_query, rec_query,
        break_offset, forget_room, out_gain.reshape(1, LANES), out_attn, out_rec,
    )
    return result.reshape(1, share, width)


def solution(mesh):
    placed = (
        P(("grp", "fs"), "sp", "tp"),
        P(),
        P("fs", "tp"),
        P("fs", "tp"),
        P("fs", "tp"),
        P("fs", "tp"),
        P("fs", "tp"),
        P("fs", "tp"),
        P("tp"),
        P("tp", None),
        P(),
        P("tp", "fs"),
        P("tp", "fs"),
    )
    return jax.shard_map(
        body,
        mesh=mesh,
        in_specs=placed,
        out_specs=P(("grp", "fs"), ("sp", "tp"), None),
        check_vma=False,
    )
```

```python
import functools
import math

import jax
import jax.numpy as jnp
from jax import lax
from jax.experimental import pallas as pl
from jax.experimental.pallas import tpu as pltpu
from jax.sharding import PartitionSpec as P

LANES = 128
norm_eps = 1e-06
MESH = pl.DeviceIdType.MESH
F32 = jnp.float32
BF16 = jnp.bfloat16
N_PROJ = 6
GROUPS = 2
CHUNKS = 2


def dot_nn(a, b):
    return lax.dot_general(a, b, (((1,), (0,)), ((), ())), preferred_element_type=F32)


def dot_nt(a, b):
    return lax.dot_general(a, b, (((1,), (1,)), ((), ())), preferred_element_type=F32)


def dot_tn(a, b):
    return lax.dot_general(a, b, (((0,), (0,)), ((), ())), preferred_element_type=F32)


def halves(x):
    high = x.astype(BF16)
    return high, (x - high.astype(F32)).astype(BF16)


def kernel(
    n_sp, n_fs, n_tp,
    tok_hbm, gain, w_k, w_v, w_f, w_i, w_q, w_r, offs, room, out_gain, o_attn, o_rec,
    out,
    tok, wbuf, obuf, xt, xg, ss, acc, psend, precv, kv, qbuf, qdec, ecum, kinv,
    att, run, loc, st_loc, dec, st_in, st_out, heads, hrecv, part_acc, part, precv2, mix, mrecv,
    t_sem, w_sem, x_send, x_recv, f_send, ss_send, ss_recv, p_send, p_recv, kv_send, kv_recv,
    st_sem, h_send, h_recv, pp_send, pp_recv, m_send, m_recv,
):
    sp, fs, tp = lax.axis_index("sp"), lax.axis_index("fs"), lax.axis_index("tp")
    rows, feat_t = tok.shape
    feat_f = xt.shape[2]
    width = feat_t * n_tp
    cols = wbuf.shape[2]
    n_heads = cols // LANES
    share = rows // n_tp
    out_cols = obuf.shape[2]
    has_next = sp < n_sp - 1
    has_prev = sp > 0

    def fs_at(step):
        return lax.rem(fs + step, n_fs)

    def tp_at(step):
        return lax.rem(tp + step, n_tp)

    tok_copy = pltpu.make_async_copy(tok_hbm, tok, t_sem.at[0])
    tok_copy.start()
    w_copies = [
        pltpu.make_async_copy(w, wbuf.at[i], w_sem.at[i])
        for i, w in enumerate((w_k, w_v, w_f, w_i, w_q, w_r))
    ]
    w_copies += [
        pltpu.make_async_copy(w, obuf.at[i], w_sem.at[N_PROJ + i])
        for i, w in enumerate((o_attn, o_rec))
    ]
    barrier = pltpu.get_barrier_semaphore()
    for df in range(n_fs):
        for dt in range(n_tp):
            if df or dt:
                pl.semaphore_signal(
                    barrier, inc=1, device_id={"fs": fs_at(df), "tp": tp_at(dt)}, device_id_type=MESH
                )

    @pl.when(has_next)
    def _():
        pl.semaphore_signal(barrier, inc=1, device_id={"sp": sp + 1}, device_id_type=MESH)

    @pl.when(has_prev)
    def _():
        pl.semaphore_signal(barrier, inc=1, device_id={"sp": sp - 1}, device_id_type=MESH)

    for copy in w_copies:
        copy.start()
    tok_copy.wait()

    next_count = jnp.where(has_next, 1, 0)
    prev_count = jnp.where(has_prev, 1, 0)
    pl.semaphore_wait(barrier, n_fs * n_tp - 1 + next_count + prev_count)

    def holder(f_index):
        return (f_index * feat_f) // feat_t

    def x_copy(df, dt):
        dest = fs_at(df)
        start = pl.multiple_of(lax.rem(dest * feat_f, feat_t), LANES)
        part_rows = rows if df == 0 else share
        first = 0 if df == 0 else pl.multiple_of(tp_at(dt) * share, share)
        piece = tp if df == 0 else tp_at(dt)
        return pltpu.make_async_remote_copy(
            src_ref=tok.at[pl.ds(first, part_rows), pl.ds(start, feat_f)],
            dst_ref=xt.at[fs, pl.ds(first, part_rows)],
            send_sem=x_send.at[df * n_tp + dt],
            recv_sem=x_recv.at[fs * n_tp + piece],
            device_id={"fs": dest, "tp": tp_at(dt)},
            device_id_type=MESH,
        )

    def f_copy(df, dt):
        slot = fs_at(df)
        first = pl.multiple_of(tp * share, share)
        return pltpu.make_async_remote_copy(
            src_ref=xt.at[slot, pl.ds(first, share)],
            dst_ref=xt.at[slot, pl.ds(first, share)],
            send_sem=f_send.at[df * n_tp + dt],
            recv_sem=x_recv.at[slot * n_tp + tp],
            device_id={"tp": tp_at(dt)},
            device_id_type=MESH,
        )

    x_order = [(df, dt) for df in list(range(1, n_fs)) + [0] for dt in range(n_tp) if df or dt]
    for df, dt in x_order:
        @pl.when(holder(fs_at(df)) == tp)
        def _(df=df, dt=dt):
            x_copy(df, dt).start()

    squares = jnp.zeros((rows, LANES), F32)
    for c in range(feat_t // LANES):
        piece = tok[:, c * LANES:(c + 1) * LANES].astype(F32)
        squares = squares + piece * piece
    ss[tp] = squares

    def ss_copy(dt):
        return pltpu.make_async_remote_copy(
            src_ref=ss.at[tp], dst_ref=ss.at[tp],
            send_sem=ss_send.at[dt - 1], recv_sem=ss_recv.at[tp],
            device_id={"tp": tp_at(dt)}, device_id_type=MESH,
        )

    for dt in range(1, n_tp):
        ss_copy(dt).start()

    own_holder = holder(fs) == tp
    gain_f = gain[:, pl.ds(pl.multiple_of(fs * feat_f, LANES), feat_f)]

    @pl.when(own_holder)
    def _():
        start = pl.multiple_of(lax.rem(fs * feat_f, feat_t), LANES)
        xg[0] = (tok[:, pl.ds(start, feat_f)].astype(F32) * gain_f).astype(BF16)

    def x_wait(slot, piece, first, count):
        view = xt.at[slot, pl.ds(first, count)]
        pltpu.make_async_remote_copy(
            src_ref=view, dst_ref=view,
            send_sem=x_send.at[0], recv_sem=x_recv.at[slot * n_tp + piece],
            device_id={"tp": tp_at(1)}, device_id_type=MESH,
        ).wait_recv()

    g_cols = cols // GROUPS
    units = [(w, g * g_cols, g_cols) for g in range(GROUPS) for w in (0, 1)]
    units += [(w, 0, cols) for w in range(2, N_PROJ)]
    n_units = len(units)
    n_kv = 2 * GROUPS

    def p_copy(df, u):
        w, first, count = units[u]
        return pltpu.make_async_remote_copy(
            src_ref=psend.at[df - 1, w, :, pl.ds(first, count)],
            dst_ref=precv.at[df - 1, w, :, pl.ds(first, count)],
            send_sem=p_send.at[(df - 1) * n_units + u], recv_sem=p_recv.at[(df - 1) * n_units + u],
            device_id={"fs": fs_at(df)}, device_id_type=MESH,
        )

    def row_part(dt):
        return pl.ds(pl.multiple_of(tp_at(dt) * share, share), share)

    def first_copy(df, dt):
        index = (n_fs - 1) * n_units + (df - 1) * n_tp + dt
        return pltpu.make_async_remote_copy(
            src_ref=psend.at[df - 1, 0, row_part(dt), pl.ds(0, g_cols)],
            dst_ref=precv.at[df - 1, 0, row_part(dt), pl.ds(0, g_cols)],
            send_sem=p_send.at[index], recv_sem=p_recv.at[index],
            device_id={"fs": fs_at(df)}, device_id_type=MESH,
        )

    def first_part(df, dt):
        mine = row_part(dt)
        xg[df, mine, :] = (xt[fs_at(df), mine, :].astype(F32) * gain_f).astype(BF16)
        psend[df - 1, 0, mine, 0:g_cols] = dot_nn(xg[df, mine, :], wbuf[0, :, 0:g_cols]).astype(BF16)
        first_copy(df, dt).start()

    w_copies[0].wait()
    for df in range(1, n_fs):
        slot = fs_at(df)
        x_wait(slot, tp, pl.multiple_of(tp * share, share), share)
        for dt in range(1, n_tp):
            f_copy(df, dt).start()
        first_part(df, 0)
    for df in range(1, n_fs):
        slot = fs_at(df)
        for dt in range(1, n_tp):
            piece = tp_at(dt)
            x_wait(slot, piece, pl.multiple_of(piece * share, share), share)
            first_part(df, dt)
    for u, (w, first, count) in enumerate(units):
        if u == 0:
            continue
        if first == 0:
            w_copies[w].wait()
        cut = slice(first, first + count)
        for df in range(1, n_fs):
            psend[df - 1, w, :, cut] = dot_nn(xg[df], wbuf[w, :, cut]).astype(BF16)
            p_copy(df, u).start()

    @pl.when(jnp.logical_not(own_holder))
    def _():
        x_wait(fs, holder(fs), 0, rows)
        xg[0] = (xt[fs].astype(F32) * gain_f).astype(BF16)

    for w in range(N_PROJ):
        acc[w] = dot_nn(xg[0], wbuf[w])

    total = ss[tp]
    for dt in range(1, n_tp):
        other = tp_at(dt)
        pltpu.make_async_remote_copy(
            src_ref=ss.at[other], dst_ref=ss.at[other],
            send_sem=ss_send.at[dt - 1], recv_sem=ss_recv.at[other],
            device_id={"tp": other}, device_id_type=MESH,
        ).wait_recv()
        total = total + ss[other]
    factor = lax.rsqrt(jnp.sum(total, axis=1, keepdims=True) / width + norm_eps)

    def finish(u):
        w, first, count = units[u]
        cut = slice(first, first + count)
        value = acc[w, :, cut]
        for df in range(1, n_fs):
            if u == 0:
                for dt in range(n_tp):
                    first_copy(df, dt).wait_recv()
            else:
                p_copy(df, u).wait_recv()
            value = value + precv[df - 1, w, :, cut].astype(F32)
        return (value * factor).astype(BF16)

    def kv_copy(slot, c):
        return pltpu.make_async_remote_copy(
            src_ref=kv.at[slot, c], dst_ref=kv.at[slot, c],
            send_sem=kv_send.at[slot * n_kv + c], recv_sem=kv_recv.at[slot * n_kv + c],
            device_id={"sp": lax.rem(sp + 1, n_sp)}, device_id_type=MESH,
        )

    for c in range(n_kv):
        kv[sp, c] = finish(c)

        @pl.when(has_next)
        def _(c=c):
            kv_copy(sp, c).start()

    def hand_on(step, c):
        kv_copy(sp - step, c).wait_recv()

        @pl.when(has_next)
        def _():
            kv_copy(sp - step, c).start()

    def hand_on_if(step, c):
        if step < n_sp:
            pl.when(sp >= step)(functools.partial(hand_on, step, c))

    hand_on_if(1, 0)
    hand_on_if(1, 1)
    iota_r = lax.broadcasted_iota(jnp.int32, (rows, rows), 0)
    iota_c = lax.broadcasted_iota(jnp.int32, (rows, rows), 1)
    causal = iota_r >= iota_c
    strict = iota_c < iota_r

    def st_copy(h):
        return pltpu.make_async_remote_copy(
            src_ref=st_out.at[h], dst_ref=st_in.at[h],
            send_sem=st_sem.at[h], recv_sem=st_sem.at[n_heads + h],
            device_id={"sp": lax.rem(sp + 1, n_sp)}, device_id_type=MESH,
        )

    lower = jnp.where(causal, 1.0, 0.0).astype(BF16)
    forget_pre = finish(n_kv)
    for c in range(2, n_kv):
        hand_on_if(1, c)
    rec_i = finish(n_kv + 1)
    for h in range(n_heads):
        lanes = slice(h * LANES, (h + 1) * LANES)
        key_in = room[h:h + 1, :] * jax.nn.sigmoid(-forget_pre[:, lanes].astype(F32))
        high, low = halves(jnp.log1p(-key_in))
        cum = dot_nn(lower, high) + dot_nn(lower, low)
        last = cum[rows - 1:rows, :]
        ecum[:, lanes] = jnp.exp(cum)
        kinv[:, lanes] = (key_in * jnp.exp(-cum)).astype(BF16)
        fresh = (key_in * jnp.exp(last - cum)).astype(BF16)
        st_loc[h] = dot_tn(rec_i[:, lanes], fresh)
        dec[h] = jnp.broadcast_to(jnp.exp(last), dec.shape[1:])

        @pl.when(jnp.logical_and(sp == 0, has_next))
        def _(h=h):
            st_out[h] = st_loc[h].astype(BF16)
            st_copy(h).start()

    hand_on_if(2, 0)
    hand_on_if(2, 1)

    qbuf[...] = finish(n_kv + 2)
    later = jnp.where(iota_r > iota_c, 1.0, 0.0).astype(BF16)
    sums = jnp.concatenate([later, jnp.ones((rows, LANES), BF16)], axis=1)
    scale = 1.0 / math.sqrt(LANES)

    g_heads = n_heads // GROUPS

    def attend(slot, g, diagonal):
        for h in range(g * g_heads, (g + 1) * g_heads):
            lanes = slice(h * LANES, (h + 1) * LANES)
            inner = slice((h - g * g_heads) * LANES, (h - g * g_heads + 1) * LANES)
            z = dot_nt(qbuf[:, lanes], kv[slot, 2 * g, :, inner]) * scale + offs[h]
            keep = -(jnp.maximum(z, 0.0) + jnp.log1p(jnp.exp(-jnp.abs(z))))
            log_stick = z + keep
            if diagonal:
                keep = jnp.where(strict, keep, 0.0)
            high, low = halves(keep)
            both = dot_nn(high, sums) + dot_nn(low, sums)
            stick = jnp.exp(log_stick + both[:, :rows])
            if diagonal:
                stick = jnp.where(strict, stick, 0.0)
            value = dot_nn(stick.astype(BF16), kv[slot, 2 * g + 1, :, inner])
            if diagonal:
                att[:, lanes] = value
                run[h] = both[:, rows:]
            else:
                past = run[h]
                att[:, lanes] += value * jnp.exp(past)
                run[h] = past + both[:, rows:]

    def attend_if(step):
        if step < n_sp:
            @pl.when(sp >= step)
            def _():
                for g in range(GROUPS):
                    attend(sp - step, g, False)

    for g in range(GROUPS):
        attend(sp, g, True)
    for c in range(2, n_kv):
        hand_on_if(2, c)
    attend_if(1)
    rec_q = finish(n_kv + 3)
    for h in range(n_heads):
        lanes = slice(h * LANES, (h + 1) * LANES)
        decayed = (rec_q[:, lanes].astype(F32) * ecum[:, lanes]).astype(BF16)
        qdec[:, lanes] = decayed
        scores = jnp.where(causal, dot_nt(decayed, kinv[:, lanes]), 0.0)
        loc[:, lanes] = dot_nn(scores.astype(BF16), rec_i[:, lanes])

    attend_if(2)

    def block(step, carry):
        for c in range(n_kv):
            hand_on(step, c)
        for g in range(GROUPS):
            attend(sp - step, g, False)
        return carry

    lax.fori_loop(3, sp, block, 0)

    n_head_units = GROUPS + n_heads

    def h_copy(df, c):
        index = (df - 1) * n_head_units + c
        if c < GROUPS:
            lanes = pl.ds(c * g_cols, g_cols)
            source, target = heads.at[0, :, lanes], hrecv.at[df - 1, 0, :, lanes]
        else:
            lanes = pl.ds((c - GROUPS) * LANES, LANES)
            source, target = heads.at[1, :, lanes], hrecv.at[df - 1, 1, :, lanes]
        return pltpu.make_async_remote_copy(
            src_ref=source, dst_ref=target, send_sem=h_send.at[index], recv_sem=h_recv.at[index],
            device_id={"fs": fs_at(df)}, device_id_type=MESH,
        )

    for g in range(GROUPS):
        @pl.when(sp >= 3)
        def _(g=g):
            for c in (2 * g, 2 * g + 1):
                hand_on(sp, c)
            attend(0, g, False)

        cut = slice(g * g_cols, (g + 1) * g_cols)
        heads[0, :, cut] = att[:, cut].astype(BF16)
        for df in range(1, n_fs):
            h_copy(df, g).start()

    for h in range(n_heads):
        lanes = slice(h * LANES, (h + 1) * LANES)

        @pl.when(has_prev)
        def _(h=h, lanes=lanes):
            st_copy(h).wait_recv()

            @pl.when(has_next)
            def _():
                st_out[h] = (st_in[h].astype(F32) * dec[h, 0:1, :] + st_loc[h]).astype(BF16)
                st_copy(h).start()

            loc[:, lanes] += dot_nt(qdec[:, lanes], st_in[h])

        raw = loc[:, lanes]
        norm = lax.rsqrt(jnp.mean(raw * raw, axis=1, keepdims=True) + norm_eps)
        heads[1, :, lanes] = (raw * norm * out_gain[...]).astype(BF16)
        for df in range(1, n_fs):
            h_copy(df, GROUPS + h).start()

    w_copies[N_PROJ].wait()
    w_copies[N_PROJ + 1].wait()

    half = out_cols // CHUNKS

    def pp_copy(df, dt, k):
        index = (df * (n_tp - 1) + dt - 1) * CHUNKS + k
        start = pl.multiple_of(tp_at(dt) * share, share)
        return pltpu.make_async_remote_copy(
            src_ref=part.at[df, k, pl.ds(start, share)], dst_ref=precv2.at[dt - 1, df, k],
            send_sem=pp_send.at[index], recv_sem=pp_recv.at[index],
            device_id={"tp": tp_at(dt)}, device_id_type=MESH,
        )

    def m_copy(df, k):
        index = (df - 1) * CHUNKS + k
        return pltpu.make_async_remote_copy(
            src_ref=mix.at[df - 1, k], dst_ref=mrecv.at[df - 1, k],
            send_sem=m_send.at[index], recv_sem=m_recv.at[index],
            device_id={"fs": fs_at(df)}, device_id_type=MESH,
        )

    def reduced(df, k):
        value = part[df, k, pl.ds(pl.multiple_of(tp * share, share), share)].astype(F32)
        for dt in range(1, n_tp):
            pp_copy(df, dt, k).wait_recv()
            value = value + precv2[dt - 1, df, k].astype(F32)
        return value.astype(BF16)

    def columns(owner, k):
        return pl.ds(pl.multiple_of(owner * out_cols + k * half, LANES), half)

    for df in range(1, n_fs):
        for g in range(GROUPS):
            h_copy(df, g).wait_recv()
        for k in range(CHUNKS):
            part_acc[df - 1, k] = dot_nn(hrecv[df - 1, 0], obuf[0, :, k * half:(k + 1) * half])
    for k in range(CHUNKS):
        cut = slice(k * half, (k + 1) * half)
        part[0, k] = (dot_nn(heads[0], obuf[0, :, cut]) + dot_nn(heads[1], obuf[1, :, cut])).astype(BF16)
        for dt in range(1, n_tp):
            pp_copy(0, dt, k).start()
    for df in range(1, n_fs):
        for h in range(n_heads):
            h_copy(df, GROUPS + h).wait_recv()
        for k in range(CHUNKS):
            cut = slice(k * half, (k + 1) * half)
            part[df, k] = (part_acc[df - 1, k] + dot_nn(hrecv[df - 1, 1], obuf[1, :, cut])).astype(BF16)
            for dt in range(1, n_tp):
                pp_copy(df, dt, k).start()
    for df in range(1, n_fs):
        for k in range(CHUNKS):
            mix[df - 1, k] = reduced(df, k)
            m_copy(df, k).start()
    for k in range(CHUNKS):
        out[:, columns(fs, k)] = reduced(0, k)
    for df in range(1, n_fs):
        source = lax.rem(fs + n_fs - df, n_fs)
        for k in range(CHUNKS):
            m_copy(df, k).wait_recv()
            out[:, columns(source, k)] = mrecv[df - 1, k]

    for df, dt in x_order:
        @pl.when(holder(fs_at(df)) == tp)
        def _(df=df, dt=dt):
            x_copy(df, dt).wait_send()
    for dt in range(1, n_tp):
        ss_copy(dt).wait_send()
        for df in range(1, n_fs):
            f_copy(df, dt).wait_send()
    for df in range(1, n_fs):
        for dt in range(n_tp):
            first_copy(df, dt).wait_send()
        for u in range(1, n_units):
            p_copy(df, u).wait_send()
        for c in range(n_head_units):
            h_copy(df, c).wait_send()
    for k in range(CHUNKS):
        for df in range(1, n_fs):
            m_copy(df, k).wait_send()
        for df in range(n_fs):
            for dt in range(1, n_tp):
                pp_copy(df, dt, k).wait_send()

    @pl.when(has_next)
    def _():
        for h in range(n_heads):
            st_copy(h).wait_send()

        def drain(slot, carry):
            for c in range(n_kv):
                kv_copy(slot, c).wait_send()
            return carry

        lax.fori_loop(0, sp + 1, drain, 0)


def body(
    tokens, mix_gain, attn_query, attn_key, attn_value, rec_query, rec_forget, rec_input,
    break_offset, forget_room, out_gain, out_attn, out_rec,
):
    n_sp, n_fs, n_tp = lax.axis_size("sp"), lax.axis_size("fs"), lax.axis_size("tp")
    rows, feat_t = tokens.shape[1], tokens.shape[2]
    feat_f, cols = attn_query.shape
    width = feat_t * n_tp
    n_heads = cols // LANES
    out_rows, out_cols = out_attn.shape
    share = rows // n_tp
    piece = out_cols // CHUNKS
    n_units = 2 * GROUPS + N_PROJ - 2
    vmem = pl.BlockSpec(memory_space=pltpu.VMEM)
    smem = pl.BlockSpec(memory_space=pltpu.SMEM)
    hbm = pl.BlockSpec(memory_space=pl.ANY)
    dma = pltpu.SemaphoreType.DMA
    square = (n_heads, LANES, LANES)
    result = pl.pallas_call(
        functools.partial(kernel, n_sp, n_fs, n_tp),
        out_shape=jax.ShapeDtypeStruct((share, width), BF16),
        in_specs=[hbm, vmem] + [hbm] * 6 + [smem, vmem, vmem, hbm, hbm],
        out_specs=vmem,
        scratch_shapes=[
            pltpu.VMEM((rows, feat_t), BF16),
            pltpu.VMEM((N_PROJ, feat_f, cols), BF16),
            pltpu.VMEM((2, out_rows, out_cols), BF16),
            pltpu.VMEM((n_fs, rows, feat_f), BF16),
            pltpu.VMEM((n_fs, rows, feat_f), BF16),
            pltpu.VMEM((n_tp, rows, LANES), F32),
            pltpu.VMEM((N_PROJ, rows, cols), F32),
            pltpu.VMEM((n_fs - 1, N_PROJ, rows, cols), BF16),
            pltpu.VMEM((n_fs - 1, N_PROJ, rows, cols), BF16),
            pltpu.VMEM((n_sp, 2 * GROUPS, rows, cols // GROUPS), BF16),
            pltpu.VMEM((rows, cols), BF16),
            pltpu.VMEM((rows, cols), BF16),
            pltpu.VMEM((rows, cols), F32),
            pltpu.VMEM((rows, cols), BF16),
            pltpu.VMEM((rows, cols), F32),
            pltpu.VMEM((n_heads, rows, LANES), F32),
            pltpu.VMEM((rows, cols), F32),
            pltpu.VMEM(square, F32),
            pltpu.VMEM((n_heads, 8, LANES), F32),
            pltpu.VMEM(square, BF16),
            pltpu.VMEM(square, BF16),
            pltpu.VMEM((2, rows, cols), BF16),
            pltpu.VMEM((n_fs - 1, 2, rows, cols), BF16),
            pltpu.VMEM((n_fs - 1, CHUNKS, rows, piece), F32),
            pltpu.VMEM((n_fs, CHUNKS, rows, piece), BF16),
            pltpu.VMEM((n_tp - 1, n_fs, CHUNKS, share, piece), BF16),
            pltpu.VMEM((n_fs - 1, CHUNKS, share, piece), BF16),
            pltpu.VMEM((n_fs - 1, CHUNKS, share, piece), BF16),
            dma((1,)), dma((N_PROJ + 2,)),
            dma((n_fs * n_tp,)), dma((n_fs * n_tp,)), dma((n_fs * n_tp,)),
            dma((n_tp - 1,)), dma((n_tp,)),
            dma(((n_fs - 1) * (n_units + n_tp),)), dma(((n_fs - 1) * (n_units + n_tp),)),
            dma((n_sp * 2 * GROUPS,)), dma((n_sp * 2 * GROUPS,)),
            dma((2 * n_heads,)),
            dma(((n_fs - 1) * (GROUPS + n_heads),)), dma(((n_fs - 1) * (GROUPS + n_heads),)),
            dma((n_fs * (n_tp - 1) * CHUNKS,)), dma((n_fs * (n_tp - 1) * CHUNKS,)),
            dma(((n_fs - 1) * CHUNKS,)), dma(((n_fs - 1) * CHUNKS,)),
        ],
        compiler_params=pltpu.CompilerParams(
            collective_id=0, has_side_effects=True, vmem_limit_bytes=60 * 1024 * 1024
        ),
        name="layer",
    )(
        tokens.reshape(rows, feat_t), mix_gain.reshape(1, width),
        attn_key, attn_value, rec_forget, rec_input, attn_query, rec_query,
        break_offset, forget_room, out_gain.reshape(1, LANES), out_attn, out_rec,
    )
    return result.reshape(1, share, width)


def solution(mesh):
    placed = (
        P(("grp", "fs"), "sp", "tp"),
        P(),
        P("fs", "tp"),
        P("fs", "tp"),
        P("fs", "tp"),
        P("fs", "tp"),
        P("fs", "tp"),
        P("fs", "tp"),
        P("tp"),
        P("tp", None),
        P(),
        P("tp", "fs"),
        P("tp", "fs"),
    )
    return jax.shard_map(
        body,
        mesh=mesh,
        in_specs=placed,
        out_specs=P(("grp", "fs"), ("sp", "tp"), None),
        check_vma=False,
    )
```

```python
import functools
import math

import jax
import jax.numpy as jnp
from jax import lax
from jax.experimental import pallas as pl
from jax.experimental.pallas import tpu as pltpu
from jax.sharding import PartitionSpec as P

LANES = 128
norm_eps = 1e-06
MESH = pl.DeviceIdType.MESH
F32 = jnp.float32
BF16 = jnp.bfloat16
N_PROJ = 6
GROUPS = 2
CHUNKS = 2


def dot_nn(a, b):
    return lax.dot_general(a, b, (((1,), (0,)), ((), ())), preferred_element_type=F32)


def dot_nt(a, b):
    return lax.dot_general(a, b, (((1,), (1,)), ((), ())), preferred_element_type=F32)


def dot_tn(a, b):
    return lax.dot_general(a, b, (((0,), (0,)), ((), ())), preferred_element_type=F32)


def halves(x):
    high = x.astype(BF16)
    return high, (x - high.astype(F32)).astype(BF16)


def kernel(
    n_sp, n_fs, n_tp,
    tok_hbm, gain, w_k, w_v, w_f, w_i, w_q, w_r, offs, room, out_gain, o_attn, o_rec,
    out,
    tok, wbuf, obuf, xt, xg, ss, acc, psend, precv, kv, qbuf, qdec, ecum, kinv,
    att, run, loc, st_loc, dec, st_in, st_out, heads, hrecv, part_acc, part, precv2, mix, mrecv,
    t_sem, w_sem, x_send, x_recv, f_send, ss_send, ss_recv, p_send, p_recv, kv_send, kv_recv,
    st_sem, h_send, h_recv, pp_send, pp_recv, m_send, m_recv,
):
    sp, fs, tp = lax.axis_index("sp"), lax.axis_index("fs"), lax.axis_index("tp")
    rows, feat_t = tok.shape
    feat_f = xt.shape[2]
    width = feat_t * n_tp
    cols = wbuf.shape[2]
    n_heads = cols // LANES
    share = rows // n_tp
    out_cols = obuf.shape[2]
    has_next = sp < n_sp - 1
    has_prev = sp > 0

    def fs_at(step):
        return lax.rem(fs + step, n_fs)

    def tp_at(step):
        return lax.rem(tp + step, n_tp)

    tok_copy = pltpu.make_async_copy(tok_hbm, tok, t_sem.at[0])
    tok_copy.start()
    w_copies = [
        pltpu.make_async_copy(w, wbuf.at[i], w_sem.at[i])
        for i, w in enumerate((w_k, w_v, w_f, w_i, w_q, w_r))
    ]
    w_copies += [
        pltpu.make_async_copy(w, obuf.at[i], w_sem.at[N_PROJ + i])
        for i, w in enumerate((o_attn, o_rec))
    ]
    barrier = pltpu.get_barrier_semaphore()
    for df in range(n_fs):
        for dt in range(n_tp):
            if df or dt:
                pl.semaphore_signal(
                    barrier, inc=1, device_id={"fs": fs_at(df), "tp": tp_at(dt)}, device_id_type=MESH
                )

    @pl.when(has_next)
    def _():
        pl.semaphore_signal(barrier, inc=1, device_id={"sp": sp + 1}, device_id_type=MESH)

    @pl.when(has_prev)
    def _():
        pl.semaphore_signal(barrier, inc=1, device_id={"sp": sp - 1}, device_id_type=MESH)

    for copy in w_copies:
        copy.start()
    tok_copy.wait()

    next_count = jnp.where(has_next, 1, 0)
    prev_count = jnp.where(has_prev, 1, 0)
    pl.semaphore_wait(barrier, n_fs * n_tp - 1 + next_count + prev_count)

    def holder(f_index):
        return (f_index * feat_f) // feat_t

    def x_copy(df, dt):
        dest = fs_at(df)
        start = pl.multiple_of(lax.rem(dest * feat_f, feat_t), LANES)
        part_rows = rows if df == 0 else share
        first = 0 if df == 0 else pl.multiple_of(tp_at(dt) * share, share)
        piece = tp if df == 0 else tp_at(dt)
        return pltpu.make_async_remote_copy(
            src_ref=tok.at[pl.ds(first, part_rows), pl.ds(start, feat_f)],
            dst_ref=xt.at[fs, pl.ds(first, part_rows)],
            send_sem=x_send.at[df * n_tp + dt],
            recv_sem=x_recv.at[fs * n_tp + piece],
            device_id={"fs": dest, "tp": tp_at(dt)},
            device_id_type=MESH,
        )

    def f_copy(df, dt):
        slot = fs_at(df)
        first = pl.multiple_of(tp * share, share)
        return pltpu.make_async_remote_copy(
            src_ref=xt.at[slot, pl.ds(first, share)],
            dst_ref=xt.at[slot, pl.ds(first, share)],
            send_sem=f_send.at[df * n_tp + dt],
            recv_sem=x_recv.at[slot * n_tp + tp],
            device_id={"tp": tp_at(dt)},
            device_id_type=MESH,
        )

    x_order = [(df, dt) for df in list(range(1, n_fs)) + [0] for dt in range(n_tp) if df or dt]
    for df, dt in x_order:
        @pl.when(holder(fs_at(df)) == tp)
        def _(df=df, dt=dt):
            x_copy(df, dt).start()

    squares = jnp.zeros((rows, LANES), F32)
    for c in range(feat_t // LANES):
        piece = tok[:, c * LANES:(c + 1) * LANES].astype(F32)
        squares = squares + piece * piece
    ss[tp] = squares

    def ss_copy(dt):
        return pltpu.make_async_remote_copy(
            src_ref=ss.at[tp], dst_ref=ss.at[tp],
            send_sem=ss_send.at[dt - 1], recv_sem=ss_recv.at[tp],
            device_id={"tp": tp_at(dt)}, device_id_type=MESH,
        )

    for dt in range(1, n_tp):
        ss_copy(dt).start()

    own_holder = holder(fs) == tp
    gain_f = gain[:, pl.ds(pl.multiple_of(fs * feat_f, LANES), feat_f)]

    @pl.when(own_holder)
    def _():
        start = pl.multiple_of(lax.rem(fs * feat_f, feat_t), LANES)
        xg[0] = (tok[:, pl.ds(start, feat_f)].astype(F32) * gain_f).astype(BF16)

    def x_wait(slot, piece, first, count):
        view = xt.at[slot, pl.ds(first, count)]
        pltpu.make_async_remote_copy(
            src_ref=view, dst_ref=view,
            send_sem=x_send.at[0], recv_sem=x_recv.at[slot * n_tp + piece],
            device_id={"tp": tp_at(1)}, device_id_type=MESH,
        ).wait_recv()

    g_cols = cols // GROUPS
    units = [(w, g * g_cols, g_cols) for g in range(GROUPS) for w in (0, 1)]
    units += [(w, 0, cols) for w in range(2, N_PROJ)]
    n_units = len(units)
    n_kv = 2 * GROUPS

    def p_copy(df, u):
        w, first, count = units[u]
        return pltpu.make_async_remote_copy(
            src_ref=psend.at[df - 1, w, :, pl.ds(first, count)],
            dst_ref=precv.at[df - 1, w, :, pl.ds(first, count)],
            send_sem=p_send.at[(df - 1) * n_units + u], recv_sem=p_recv.at[(df - 1) * n_units + u],
            device_id={"fs": fs_at(df)}, device_id_type=MESH,
        )

    def row_part(dt):
        return pl.ds(pl.multiple_of(tp_at(dt) * share, share), share)

    def first_copy(df, dt):
        index = (n_fs - 1) * n_units + (df - 1) * n_tp + dt
        return pltpu.make_async_remote_copy(
            src_ref=psend.at[df - 1, 0, row_part(dt), pl.ds(0, g_cols)],
            dst_ref=precv.at[df - 1, 0, row_part(dt), pl.ds(0, g_cols)],
            send_sem=p_send.at[index], recv_sem=p_recv.at[index],
            device_id={"fs": fs_at(df)}, device_id_type=MESH,
        )

    def first_part(df, dt):
        mine = row_part(dt)
        xg[df, mine, :] = (xt[fs_at(df), mine, :].astype(F32) * gain_f).astype(BF16)
        psend[df - 1, 0, mine, 0:g_cols] = dot_nn(xg[df, mine, :], wbuf[0, :, 0:g_cols]).astype(BF16)
        first_copy(df, dt).start()

    w_copies[0].wait()
    for df in range(1, n_fs):
        slot = fs_at(df)
        x_wait(slot, tp, pl.multiple_of(tp * share, share), share)
        for dt in range(1, n_tp):
            f_copy(df, dt).start()
        first_part(df, 0)
    for df in range(1, n_fs):
        slot = fs_at(df)
        for dt in range(1, n_tp):
            piece = tp_at(dt)
            x_wait(slot, piece, pl.multiple_of(piece * share, share), share)
            first_part(df, dt)
    for u, (w, first, count) in enumerate(units):
        if u == 0:
            continue
        if first == 0:
            w_copies[w].wait()
        cut = slice(first, first + count)
        for df in range(1, n_fs):
            psend[df - 1, w, :, cut] = dot_nn(xg[df], wbuf[w, :, cut]).astype(BF16)
            p_copy(df, u).start()

    @pl.when(jnp.logical_not(own_holder))
    def _():
        x_wait(fs, holder(fs), 0, rows)
        xg[0] = (xt[fs].astype(F32) * gain_f).astype(BF16)

    for w in range(2):
        acc[w] = dot_nn(xg[0], wbuf[w])

    total = ss[tp]
    for dt in range(1, n_tp):
        other = tp_at(dt)
        pltpu.make_async_remote_copy(
            src_ref=ss.at[other], dst_ref=ss.at[other],
            send_sem=ss_send.at[dt - 1], recv_sem=ss_recv.at[other],
            device_id={"tp": other}, device_id_type=MESH,
        ).wait_recv()
        total = total + ss[other]
    factor = lax.rsqrt(jnp.sum(total, axis=1, keepdims=True) / width + norm_eps)

    def finish(u):
        w, first, count = units[u]
        cut = slice(first, first + count)
        value = acc[w, :, cut]
        for df in range(1, n_fs):
            if u == 0:
                for dt in range(n_tp):
                    first_copy(df, dt).wait_recv()
            else:
                p_copy(df, u).wait_recv()
            value = value + precv[df - 1, w, :, cut].astype(F32)
        return (value * factor).astype(BF16)

    def kv_copy(slot, c):
        return pltpu.make_async_remote_copy(
            src_ref=kv.at[slot, c], dst_ref=kv.at[slot, c],
            send_sem=kv_send.at[slot * n_kv + c], recv_sem=kv_recv.at[slot * n_kv + c],
            device_id={"sp": lax.rem(sp + 1, n_sp)}, device_id_type=MESH,
        )

    for c in range(n_kv):
        kv[sp, c] = finish(c)

        @pl.when(has_next)
        def _(c=c):
            kv_copy(sp, c).start()

    for w in range(2, N_PROJ):
        acc[w] = dot_nn(xg[0], wbuf[w])

    def hand_on(step, c):
        kv_copy(sp - step, c).wait_recv()

        @pl.when(has_next)
        def _():
            kv_copy(sp - step, c).start()

    def hand_on_if(step, c):
        if step < n_sp:
            pl.when(sp >= step)(functools.partial(hand_on, step, c))

    hand_on_if(1, 0)
    hand_on_if(1, 1)
    iota_r = lax.broadcasted_iota(jnp.int32, (rows, rows), 0)
    iota_c = lax.broadcasted_iota(jnp.int32, (rows, rows), 1)
    causal = iota_r >= iota_c
    strict = iota_c < iota_r

    def st_copy(h):
        return pltpu.make_async_remote_copy(
            src_ref=st_out.at[h], dst_ref=st_in.at[h],
            send_sem=st_sem.at[h], recv_sem=st_sem.at[n_heads + h],
            device_id={"sp": lax.rem(sp + 1, n_sp)}, device_id_type=MESH,
        )

    lower = jnp.where(causal, 1.0, 0.0).astype(BF16)
    forget_pre = finish(n_kv)
    for c in range(2, n_kv):
        hand_on_if(1, c)
    rec_i = finish(n_kv + 1)
    for h in range(n_heads):
        lanes = slice(h * LANES, (h + 1) * LANES)
        key_in = room[h:h + 1, :] * jax.nn.sigmoid(-forget_pre[:, lanes].astype(F32))
        high, low = halves(jnp.log1p(-key_in))
        cum = dot_nn(lower, high) + dot_nn(lower, low)
        last = cum[rows - 1:rows, :]
        ecum[:, lanes] = jnp.exp(cum)
        kinv[:, lanes] = (key_in * jnp.exp(-cum)).astype(BF16)
        fresh = (key_in * jnp.exp(last - cum)).astype(BF16)
        st_loc[h] = dot_tn(rec_i[:, lanes], fresh)
        dec[h] = jnp.broadcast_to(jnp.exp(last), dec.shape[1:])

        @pl.when(jnp.logical_and(sp == 0, has_next))
        def _(h=h):
            st_out[h] = st_loc[h].astype(BF16)
            st_copy(h).start()

    hand_on_if(2, 0)
    hand_on_if(2, 1)

    qbuf[...] = finish(n_kv + 2)
    later = jnp.where(iota_r > iota_c, 1.0, 0.0).astype(BF16)
    sums = jnp.concatenate([later, jnp.ones((rows, LANES), BF16)], axis=1)
    scale = 1.0 / math.sqrt(LANES)

    g_heads = n_heads // GROUPS

    def attend(slot, g, diagonal):
        for h in range(g * g_heads, (g + 1) * g_heads):
            lanes = slice(h * LANES, (h + 1) * LANES)
            inner = slice((h - g * g_heads) * LANES, (h - g * g_heads + 1) * LANES)
            z = dot_nt(qbuf[:, lanes], kv[slot, 2 * g, :, inner]) * scale + offs[h]
            keep = -(jnp.maximum(z, 0.0) + jnp.log1p(jnp.exp(-jnp.abs(z))))
            log_stick = z + keep
            if diagonal:
                keep = jnp.where(strict, keep, 0.0)
            high, low = halves(keep)
            both = dot_nn(high, sums) + dot_nn(low, sums)
            stick = jnp.exp(log_stick + both[:, :rows])
            if diagonal:
                stick = jnp.where(strict, stick, 0.0)
            value = dot_nn(stick.astype(BF16), kv[slot, 2 * g + 1, :, inner])
            if diagonal:
                att[:, lanes] = value
                run[h] = both[:, rows:]
            else:
                past = run[h]
                att[:, lanes] += value * jnp.exp(past)
                run[h] = past + both[:, rows:]

    def attend_if(step):
        if step < n_sp:
            @pl.when(sp >= step)
            def _():
                for g in range(GROUPS):
                    attend(sp - step, g, False)

    for g in range(GROUPS):
        attend(sp, g, True)
    for c in range(2, n_kv):
        hand_on_if(2, c)
    attend_if(1)
    rec_q = finish(n_kv + 3)
    for h in range(n_heads):
        lanes = slice(h * LANES, (h + 1) * LANES)
        decayed = (rec_q[:, lanes].astype(F32) * ecum[:, lanes]).astype(BF16)
        qdec[:, lanes] = decayed
        scores = jnp.where(causal, dot_nt(decayed, kinv[:, lanes]), 0.0)
        loc[:, lanes] = dot_nn(scores.astype(BF16), rec_i[:, lanes])

    attend_if(2)

    def block(step, carry):
        for c in range(n_kv):
            hand_on(step, c)
        for g in range(GROUPS):
            attend(sp - step, g, False)
        return carry

    lax.fori_loop(3, sp, block, 0)

    n_head_units = GROUPS + n_heads

    def h_copy(df, c):
        index = (df - 1) * n_head_units + c
        if c < GROUPS:
            lanes = pl.ds(c * g_cols, g_cols)
            source, target = heads.at[0, :, lanes], hrecv.at[df - 1, 0, :, lanes]
        else:
            lanes = pl.ds((c - GROUPS) * LANES, LANES)
            source, target = heads.at[1, :, lanes], hrecv.at[df - 1, 1, :, lanes]
        return pltpu.make_async_remote_copy(
            src_ref=source, dst_ref=target, send_sem=h_send.at[index], recv_sem=h_recv.at[index],
            device_id={"fs": fs_at(df)}, device_id_type=MESH,
        )

    for g in range(GROUPS):
        @pl.when(sp >= 3)
        def _(g=g):
            for c in (2 * g, 2 * g + 1):
                hand_on(sp, c)
            attend(0, g, False)

        cut = slice(g * g_cols, (g + 1) * g_cols)
        heads[0, :, cut] = att[:, cut].astype(BF16)
        for df in range(1, n_fs):
            h_copy(df, g).start()

    for h in range(n_heads):
        lanes = slice(h * LANES, (h + 1) * LANES)

        @pl.when(has_prev)
        def _(h=h, lanes=lanes):
            st_copy(h).wait_recv()

            @pl.when(has_next)
            def _():
                st_out[h] = (st_in[h].astype(F32) * dec[h, 0:1, :] + st_loc[h]).astype(BF16)
                st_copy(h).start()

            loc[:, lanes] += dot_nt(qdec[:, lanes], st_in[h])

        raw = loc[:, lanes]
        norm = lax.rsqrt(jnp.mean(raw * raw, axis=1, keepdims=True) + norm_eps)
        heads[1, :, lanes] = (raw * norm * out_gain[...]).astype(BF16)
        for df in range(1, n_fs):
            h_copy(df, GROUPS + h).start()

    w_copies[N_PROJ].wait()
    w_copies[N_PROJ + 1].wait()

    half = out_cols // CHUNKS

    def pp_copy(df, dt, k):
        index = (df * (n_tp - 1) + dt - 1) * CHUNKS + k
        start = pl.multiple_of(tp_at(dt) * share, share)
        return pltpu.make_async_remote_copy(
            src_ref=part.at[df, k, pl.ds(start, share)], dst_ref=precv2.at[dt - 1, df, k],
            send_sem=pp_send.at[index], recv_sem=pp_recv.at[index],
            device_id={"tp": tp_at(dt)}, device_id_type=MESH,
        )

    def m_copy(df, k):
        index = (df - 1) * CHUNKS + k
        return pltpu.make_async_remote_copy(
            src_ref=mix.at[df - 1, k], dst_ref=mrecv.at[df - 1, k],
            send_sem=m_send.at[index], recv_sem=m_recv.at[index],
            device_id={"fs": fs_at(df)}, device_id_type=MESH,
        )

    def reduced(df, k):
        value = part[df, k, pl.ds(pl.multiple_of(tp * share, share), share)].astype(F32)
        for dt in range(1, n_tp):
            pp_copy(df, dt, k).wait_recv()
            value = value + precv2[dt - 1, df, k].astype(F32)
        return value.astype(BF16)

    def columns(owner, k):
        return pl.ds(pl.multiple_of(owner * out_cols + k * half, LANES), half)

    for df in range(1, n_fs):
        for g in range(GROUPS):
            h_copy(df, g).wait_recv()
        for k in range(CHUNKS):
            part_acc[df - 1, k] = dot_nn(hrecv[df - 1, 0], obuf[0, :, k * half:(k + 1) * half])
    for k in range(CHUNKS):
        cut = slice(k * half, (k + 1) * half)
        part[0, k] = (dot_nn(heads[0], obuf[0, :, cut]) + dot_nn(heads[1], obuf[1, :, cut])).astype(BF16)
        for dt in range(1, n_tp):
            pp_copy(0, dt, k).start()
    for df in range(1, n_fs):
        for h in range(n_heads):
            h_copy(df, GROUPS + h).wait_recv()
        for k in range(CHUNKS):
            cut = slice(k * half, (k + 1) * half)
            part[df, k] = (part_acc[df - 1, k] + dot_nn(hrecv[df - 1, 1], obuf[1, :, cut])).astype(BF16)
            for dt in range(1, n_tp):
                pp_copy(df, dt, k).start()
    for df in range(1, n_fs):
        for k in range(CHUNKS):
            mix[df - 1, k] = reduced(df, k)
            m_copy(df, k).start()
    for k in range(CHUNKS):
        out[:, columns(fs, k)] = reduced(0, k)
    for df in range(1, n_fs):
        source = lax.rem(fs + n_fs - df, n_fs)
        for k in range(CHUNKS):
            m_copy(df, k).wait_recv()
            out[:, columns(source, k)] = mrecv[df - 1, k]

    for df, dt in x_order:
        @pl.when(holder(fs_at(df)) == tp)
        def _(df=df, dt=dt):
            x_copy(df, dt).wait_send()
    for dt in range(1, n_tp):
        ss_copy(dt).wait_send()
        for df in range(1, n_fs):
            f_copy(df, dt).wait_send()
    for df in range(1, n_fs):
        for dt in range(n_tp):
            first_copy(df, dt).wait_send()
        for u in range(1, n_units):
            p_copy(df, u).wait_send()
        for c in range(n_head_units):
            h_copy(df, c).wait_send()
    for k in range(CHUNKS):
        for df in range(1, n_fs):
            m_copy(df, k).wait_send()
        for df in range(n_fs):
            for dt in range(1, n_tp):
                pp_copy(df, dt, k).wait_send()

    @pl.when(has_next)
    def _():
        for h in range(n_heads):
            st_copy(h).wait_send()

        def drain(slot, carry):
            for c in range(n_kv):
                kv_copy(slot, c).wait_send()
            return carry

        lax.fori_loop(0, sp + 1, drain, 0)


def body(
    tokens, mix_gain, attn_query, attn_key, attn_value, rec_query, rec_forget, rec_input,
    break_offset, forget_room, out_gain, out_attn, out_rec,
):
    n_sp, n_fs, n_tp = lax.axis_size("sp"), lax.axis_size("fs"), lax.axis_size("tp")
    rows, feat_t = tokens.shape[1], tokens.shape[2]
    feat_f, cols = attn_query.shape
    width = feat_t * n_tp
    n_heads = cols // LANES
    out_rows, out_cols = out_attn.shape
    share = rows // n_tp
    piece = out_cols // CHUNKS
    n_units = 2 * GROUPS + N_PROJ - 2
    vmem = pl.BlockSpec(memory_space=pltpu.VMEM)
    smem = pl.BlockSpec(memory_space=pltpu.SMEM)
    hbm = pl.BlockSpec(memory_space=pl.ANY)
    dma = pltpu.SemaphoreType.DMA
    square = (n_heads, LANES, LANES)
    result = pl.pallas_call(
        functools.partial(kernel, n_sp, n_fs, n_tp),
        out_shape=jax.ShapeDtypeStruct((share, width), BF16),
        in_specs=[hbm, vmem] + [hbm] * 6 + [smem, vmem, vmem, hbm, hbm],
        out_specs=vmem,
        scratch_shapes=[
            pltpu.VMEM((rows, feat_t), BF16),
            pltpu.VMEM((N_PROJ, feat_f, cols), BF16),
            pltpu.VMEM((2, out_rows, out_cols), BF16),
            pltpu.VMEM((n_fs, rows, feat_f), BF16),
            pltpu.VMEM((n_fs, rows, feat_f), BF16),
            pltpu.VMEM((n_tp, rows, LANES), F32),
            pltpu.VMEM((N_PROJ, rows, cols), F32),
            pltpu.VMEM((n_fs - 1, N_PROJ, rows, cols), BF16),
            pltpu.VMEM((n_fs - 1, N_PROJ, rows, cols), BF16),
            pltpu.VMEM((n_sp, 2 * GROUPS, rows, cols // GROUPS), BF16),
            pltpu.VMEM((rows, cols), BF16),
            pltpu.VMEM((rows, cols), BF16),
            pltpu.VMEM((rows, cols), F32),
            pltpu.VMEM((rows, cols), BF16),
            pltpu.VMEM((rows, cols), F32),
            pltpu.VMEM((n_heads, rows, LANES), F32),
            pltpu.VMEM((rows, cols), F32),
            pltpu.VMEM(square, F32),
            pltpu.VMEM((n_heads, 8, LANES), F32),
            pltpu.VMEM(square, BF16),
            pltpu.VMEM(square, BF16),
            pltpu.VMEM((2, rows, cols), BF16),
            pltpu.VMEM((n_fs - 1, 2, rows, cols), BF16),
            pltpu.VMEM((n_fs - 1, CHUNKS, rows, piece), F32),
            pltpu.VMEM((n_fs, CHUNKS, rows, piece), BF16),
            pltpu.VMEM((n_tp - 1, n_fs, CHUNKS, share, piece), BF16),
            pltpu.VMEM((n_fs - 1, CHUNKS, share, piece), BF16),
            pltpu.VMEM((n_fs - 1, CHUNKS, share, piece), BF16),
            dma((1,)), dma((N_PROJ + 2,)),
            dma((n_fs * n_tp,)), dma((n_fs * n_tp,)), dma((n_fs * n_tp,)),
            dma((n_tp - 1,)), dma((n_tp,)),
            dma(((n_fs - 1) * (n_units + n_tp),)), dma(((n_fs - 1) * (n_units + n_tp),)),
            dma((n_sp * 2 * GROUPS,)), dma((n_sp * 2 * GROUPS,)),
            dma((2 * n_heads,)),
            dma(((n_fs - 1) * (GROUPS + n_heads),)), dma(((n_fs - 1) * (GROUPS + n_heads),)),
            dma((n_fs * (n_tp - 1) * CHUNKS,)), dma((n_fs * (n_tp - 1) * CHUNKS,)),
            dma(((n_fs - 1) * CHUNKS,)), dma(((n_fs - 1) * CHUNKS,)),
        ],
        compiler_params=pltpu.CompilerParams(
            collective_id=0, has_side_effects=True, vmem_limit_bytes=60 * 1024 * 1024
        ),
        name="layer",
    )(
        tokens.reshape(rows, feat_t), mix_gain.reshape(1, width),
        attn_key, attn_value, rec_forget, rec_input, attn_query, rec_query,
        break_offset, forget_room, out_gain.reshape(1, LANES), out_attn, out_rec,
    )
    return result.reshape(1, share, width)


def solution(mesh):
    placed = (
        P(("grp", "fs"), "sp", "tp"),
        P(),
        P("fs", "tp"),
        P("fs", "tp"),
        P("fs", "tp"),
        P("fs", "tp"),
        P("fs", "tp"),
        P("fs", "tp"),
        P("tp"),
        P("tp", None),
        P(),
        P("tp", "fs"),
        P("tp", "fs"),
    )
    return jax.shard_map(
        body,
        mesh=mesh,
        in_specs=placed,
        out_specs=P(("grp", "fs"), ("sp", "tp"), None),
        check_vma=False,
    )
```
